32 devices in a mesh: sp: 8 (over z, y), tp: 4 (over x, core).
Axes of the slice: x: 2, y: 2, z: 4, core: 2. Of those that a mesh axis runs over, the one named last changes fastest.
Arguments:
- tokens: bfloat16 [2048, 2048], P('sp'), may hold values from -6 to 6
- input_norm_gain: float32 [2048], replicated, may hold values from 0.1 to 1.9
- convolution_value_weight: bfloat16 [2048, 512], P(None, 'tp'), may hold values from -0.125 to 0.125
- convolution_gate_weight: bfloat16 [2048, 512], P(None, 'tp'), may hold values from -0.125 to 0.125
- depthwise_taps_weight: float32 [31, 512], P(None, 'tp'), may hold values from -1 to 1
- convolution_group_gain: float32 [512], P('tp'), may hold values from 0.1 to 1.9
- convolution_group_shift: float32 [512], P('tp'), may hold values from -3 to 3
- receptance_weight: bfloat16 [2048, 1024], P(None, 'tp'), may hold values from -0.125 to 0.125
- key_weight: bfloat16 [2048, 1024], P(None, 'tp'), may hold values from -0.125 to 0.125
- value_weight: bfloat16 [2048, 1024], P(None, 'tp'), may hold values from -0.125 to 0.125
- decay_weight: bfloat16 [2048, 1024], P(None, 'tp'), may hold values from -0.0625 to 0.0625
- correction_rate_weight: bfloat16 [2048, 1024], P(None, 'tp'), may hold values from -0.125 to 0.125
- output_gate_weight: bfloat16 [2048, 1024], P(None, 'tp'), may hold values from -0.125 to 0.125
- key_prenorm_gain: float32 [1024], P('tp'), may hold values from 0.04 to 8
- decay_offset_bias: float32 [1024], P('tp'), may hold values from -30 to 0
- position_decay_shift: float32 [2048, 1024], P('sp', 'tp'), may hold values from -1 to 1
- extra_log_decay: float32 [2048, 1024], P('sp', 'tp'), may hold values from -0.7 to 0
- head_norm_gain: float32 [1024], P('tp'), may hold values from 0.1 to 1.9
- convolution_output_weight: bfloat16 [512, 2048], replicated, may hold values from -0.15625 to 0.15625
- attention_output_weight: bfloat16 [1024, 2048], replicated, may hold values from -0.15625 to 0.15625
Outputs:
- mixed: bfloat16 [2048, 2048], P(('sp', 'tp'))
The draws below stay inside these ranges and needn't reach their ends.
All inputs are finite; a program needn't handle non-finite values.
Results may differ from the reference program's by a relative error of at most 0.0063.
The reference program's roundings to bfloat16 on the way (of `normed`, `conv_input`, `conv_out` and `mix_out`) count: a program that leaves them out, or rounds other values in their place, can miss the bound.
Values may be sent and summed in bfloat16 or wider, within the bound.
A program may use at most 128 MiB of HBM per device.

```python
import jax
import jax.numpy as jnp
from jax import lax

D = 2048
CONV_CH = 512
CONV_TAPS = 31
HEADS = 16
HEAD = 64
TOKENS = 2048
MIX_CH = 1024


def draw_key_prenorm_gain(key, part):
    second = jax.random.fold_in(jax.random.fold_in(key, 53), 1)
    gain = jnp.exp(jnp.log(0.04) + jnp.log(200.0) * jax.random.uniform(second, (HEADS * HEAD,)))
    return jnp.clip(gain, 0.04, 8.0).astype(jnp.float32)


def draw_decay_offset_bias(key, part):
    first, second, third, fourth = jax.random.split(jax.random.fold_in(key, 11), 4)
    share = 0.5
    slow_head = jax.random.uniform(first, (HEADS,)) < share
    keep_scale = jnp.exp(jnp.log(0.1) + jnp.log(6.0) * jax.random.uniform(second, (HEADS,)))
    fast_length = jax.random.uniform(third, (HEADS,), minval=25.0, maxval=50.0)
    level = jnp.where(slow_head, jnp.log(keep_scale / TOKENS), -jnp.log(fast_length)) + 0.5
    jitter = jnp.clip(0.3 * jax.random.normal(fourth, (HEADS, HEAD)), -1.0, 1.0)
    return (level[:, None] + jitter).reshape(HEADS * HEAD).astype(jnp.float32)


def draw_position_decay_shift(key, part):
    level_key = jax.random.fold_in(key, 23)
    block_count = (TOKENS + 127) // 128
    level = jax.random.uniform(level_key, (block_count, HEADS), minval=-0.7, maxval=0.7)
    spread_rows = jnp.repeat(level, 128, axis=0)[:TOKENS]
    return jnp.repeat(spread_rows, HEAD, axis=1).astype(jnp.float32)


def draw_extra_log_decay(key, part):
    first, second = jax.random.split(jax.random.fold_in(key, 37), 2)
    places = jax.random.randint(first, (6,), 0, TOKENS)
    kept = jax.random.uniform(second, (6, HEADS * HEAD), minval=0.5, maxval=0.8)
    return jnp.zeros((TOKENS, HEADS * HEAD), jnp.float32).at[places].min(jnp.log(kept))


def level_of(stream_key, dims, pieces, smallest, top_value):
    def one(dim, shards_of):
        draws = jax.random.uniform(jax.random.fold_in(jax.random.fold_in(stream_key, 6), dim), (shards_of,), jnp.float32, smallest / len(pieces), top_value / len(pieces))
        return jnp.repeat(jnp.exp(draws), dims[dim] // shards_of).reshape((-1,) + (1,) * (len(dims) - dim - 1))

    factor_of = one(*pieces[0])
    for cut in pieces[1:]:
        factor_of = factor_of * one(*cut)
    return factor_of


def normal_values(rng, extent, spread, limit, cuts=(), kind=jnp.bfloat16):
    entries = spread * jax.random.normal(rng, extent, jnp.float32)
    if cuts:
        entries = entries * level_of(rng, extent, cuts, -0.22, 0.18)
    return jnp.clip(entries, -limit, limit).astype(kind)


def setup_inputs(seed: int = 0) -> dict:
    splits = jax.random.split(jax.random.key(seed), 21)
    tokens = normal_values(splits[0], (TOKENS, D), 1.0, 6.0, ((0, 8),))
    input_norm_gain = jnp.clip(1.0 + 0.18 * jax.random.normal(splits[1], (D,), jnp.float32), 0.1, 1.9)
    convolution_value_weight = normal_values(splits[2], (D, CONV_CH), D ** -0.5, 0.125, ((1, 4),))
    convolution_gate_weight = normal_values(splits[3], (D, CONV_CH), D ** -0.5, 0.125, ((1, 4),))
    depthwise_taps_weight = normal_values(splits[4], (CONV_TAPS, CONV_CH), CONV_TAPS ** -0.5, 1.0, ((1, 4),), jnp.float32)
    convolution_group_gain = jnp.clip(1.0 + 0.18 * jax.random.normal(splits[5], (CONV_CH,), jnp.float32), 0.1, 1.9)
    convolution_group_shift = normal_values(splits[6], (CONV_CH,), 0.5, 3.0, ((0, 4),), jnp.float32)
    receptance_weight = normal_values(splits[7], (D, MIX_CH), D ** -0.5, 0.125, ((1, 4),))
    key_weight = normal_values(splits[8], (D, MIX_CH), D ** -0.5, 0.125, ((1, 4),))
    value_weight = normal_values(splits[9], (D, MIX_CH), D ** -0.5, 0.125, ((1, 4),))
    decay_weight = normal_values(splits[10], (D, MIX_CH), (4 * D) ** -0.5, 0.0625, ((1, 4),))
    correction_rate_weight = normal_values(splits[11], (D, MIX_CH), D ** -0.5, 0.125, ((1, 4),))
    output_gate_weight = normal_values(splits[12], (D, MIX_CH), D ** -0.5, 0.125, ((1, 4),))
    key_prenorm_gain = draw_key_prenorm_gain(jax.random.fold_in(splits[20], 71), 0)
    decay_offset_bias = draw_decay_offset_bias(jax.random.fold_in(splits[20], 71), 0)
    position_decay_shift = draw_position_decay_shift(jax.random.fold_in(splits[20], 71), 0)
    extra_log_decay = draw_extra_log_decay(jax.random.fold_in(splits[20], 71), 0)
    head_norm_gain = jnp.clip(1.0 + 0.18 * jax.random.normal(splits[17], (MIX_CH,), jnp.float32), 0.1, 1.9)
    convolution_output_weight = normal_values(splits[18], (CONV_CH, D), (CONV_CH + MIX_CH) ** -0.5, 0.15625)
    attention_output_weight = normal_values(splits[19], (MIX_CH, D), (CONV_CH + MIX_CH) ** -0.5, 0.15625)
    return dict(tokens=tokens, input_norm_gain=input_norm_gain, convolution_value_weight=convolution_value_weight, convolution_gate_weight=convolution_gate_weight, depthwise_taps_weight=depthwise_taps_weight, convolution_group_gain=convolution_group_gain, convolution_group_shift=convolution_group_shift, receptance_weight=receptance_weight, key_weight=key_weight, value_weight=value_weight, decay_weight=decay_weight, correction_rate_weight=correction_rate_weight, output_gate_weight=output_gate_weight, key_prenorm_gain=key_prenorm_gain, decay_offset_bias=decay_offset_bias, position_decay_shift=position_decay_shift, extra_log_decay=extra_log_decay, head_norm_gain=head_norm_gain, convolution_output_weight=convolution_output_weight, attention_output_weight=attention_output_weight)


NORM_EPS = 1e-06
GROUP_EPS = 1e-05
HEAD_EPS = 0.00064
KEY_EPS = 1e-06

def stored(values):
    return lax.optimization_barrier(values.astype(jnp.bfloat16)).astype(jnp.float32)

def recurrence_step(state, inputs):
    receptance, decay, key_row, value_row, unit_key, erase_dir = inputs
    removed = jnp.einsum('hij,hj->hi', state, -unit_key)
    state = state * decay[:, None, :] + removed[:, :, None] * erase_dir[:, None, :] + value_row[:, :, None] * key_row[:, None, :]
    return (state, jnp.einsum('hij,hj->hi', state, receptance))

def reference(tokens, input_norm_gain, convolution_value_weight, convolution_gate_weight, depthwise_taps_weight, convolution_group_gain, convolution_group_shift, receptance_weight, key_weight, value_weight, decay_weight, correction_rate_weight, output_gate_weight, key_prenorm_gain, decay_offset_bias, position_decay_shift, extra_log_decay, head_norm_gain, convolution_output_weight, attention_output_weight):
    float_rows = tokens.astype(jnp.float32)
    normed = (float_rows * lax.rsqrt(lax.optimization_barrier(jnp.mean(float_rows * float_rows, axis=-1, keepdims=True)) + NORM_EPS) * input_norm_gain).astype(jnp.bfloat16)

    def project(weight):
        return stored(jnp.dot(normed, weight, preferred_element_type=jnp.float32))
    conv_input = stored(project(convolution_value_weight) * jax.nn.sigmoid(project(convolution_gate_weight)))
    padded = jnp.pad(conv_input, ((CONV_TAPS - 1, 0), (0, 0)))
    conv_sum = jnp.zeros((TOKENS, CONV_CH), jnp.float32)
    for offset in range(CONV_TAPS):
        conv_sum = conv_sum + depthwise_taps_weight[offset] * padded[offset:offset + TOKENS]
    grouped = conv_sum.reshape(TOKENS, CONV_CH // 64, 64)
    centred = grouped - lax.optimization_barrier(jnp.mean(grouped, axis=-1, keepdims=True))
    grouped = centred * lax.rsqrt(lax.optimization_barrier(jnp.mean(centred * centred, axis=-1, keepdims=True)) + GROUP_EPS)
    conv_out = jax.nn.silu(grouped.reshape(TOKENS, CONV_CH) * convolution_group_gain + convolution_group_shift).astype(jnp.bfloat16)
    receptance = project(receptance_weight)
    key_all = project(key_weight)
    value_all = project(value_weight)
    decay_logits = project(decay_weight) + decay_offset_bias + position_decay_shift
    decay_logarithm = -jnp.exp(-jax.nn.softplus(-decay_logits) - 0.5) + extra_log_decay
    erase_rate = jax.nn.sigmoid(project(correction_rate_weight))
    out_gate = jax.nn.sigmoid(project(output_gate_weight))

    def by_head(values):
        return values.reshape(TOKENS, HEADS, HEAD)
    unit_key = by_head(key_all * key_prenorm_gain)
    unit_key = unit_key * lax.rsqrt(lax.optimization_barrier(jnp.sum(unit_key * unit_key, axis=-1, keepdims=True)) + KEY_EPS)
    erase_dir = unit_key * by_head(erase_rate)
    start_state = jnp.zeros((HEADS, HEAD, HEAD), jnp.float32)
    _, readout = lax.scan(recurrence_step, start_state, (by_head(receptance), by_head(jnp.exp(decay_logarithm)), by_head(key_all), by_head(value_all), unit_key, erase_dir))
    centred_read = readout - lax.optimization_barrier(jnp.mean(readout, axis=-1, keepdims=True))
    normed_read = centred_read * lax.rsqrt(lax.optimization_barrier(jnp.mean(centred_read * centred_read, axis=-1, keepdims=True)) + HEAD_EPS)
    mix_out = (normed_read.reshape(TOKENS, HEADS * HEAD) * head_norm_gain * out_gate).astype(jnp.bfloat16)
    projected = jnp.dot(conv_out, convolution_output_weight, preferred_element_type=jnp.float32) + jnp.dot(mix_out, attention_output_weight, preferred_element_type=jnp.float32)
    return projected.astype(jnp.bfloat16)
```

```python
import functools

import jax
import jax.numpy as jnp
from jax import lax
from jax.experimental import pallas as pl
from jax.experimental.pallas import tpu as pltpu
from jax.sharding import PartitionSpec as P

HEAD = 64
CHUNK = 64
PAIR = 128

NORM_EPS = 1e-06
GROUP_EPS = 1e-05
HEAD_EPS = 0.00064
KEY_EPS = 1e-06
MESH = pl.DeviceIdType.MESH
WIRE = jnp.bfloat16
VMEM_LIMIT = 60 * 1024 * 1024
F32 = jnp.float32
BF16 = jnp.bfloat16

NN = (((1,), (0,)), ((), ()))
NT = (((1,), (1,)), ((), ()))
TN = (((0,), (0,)), ((), ()))


def parts(x, count):
    out = []
    for _ in range(count - 1):
        piece = x.astype(BF16)
        out.append(piece)
        x = x - piece.astype(F32)
    out.append(x.astype(BF16))
    return out


def dot(a, b, dims=NN):
    return lax.dot_general(a, b, dims, preferred_element_type=F32)


def mm3(a, b, dims=NN):
    ah, al = parts(a, 2)
    bh, bl = parts(b, 2)
    return dot(ah, bh, dims) + (dot(ah, bl, dims) + dot(al, bh, dims))


def mm_left(a, b, dims=NN, count=2):
    pieces = [dot(piece, b, dims) for piece in parts(a, count)]
    return functools.reduce(jnp.add, pieces)


def mm_right(a, b, dims=NN, count=2):
    pieces = [dot(a, piece, dims) for piece in parts(b, count)]
    return functools.reduce(jnp.add, pieces)


PASSES = dict(qk=3, kmv=2, inv=1, rem=1, res=3, fix=1, read=3, keep=3, state=3, carry=3, enter=3)
REFINE = True


def mm(a, b, site, dims=NN):
    passes = PASSES[site]
    if passes == 1:
        return dot(a.astype(BF16), b.astype(BF16), dims)
    if passes == 2:
        return mm_left(a, b.astype(BF16), dims)
    return mm3(a, b, dims)


def iota2(rows, cols):
    return (
        lax.broadcasted_iota(jnp.int32, (rows, cols), 0),
        lax.broadcasted_iota(jnp.int32, (rows, cols), 1),
    )


def head_blocks(width):
    row, col = iota2(width, width)
    return (row // HEAD) == (col // HEAD)


def block_diagonal(stacked, width):
    tiled = jnp.concatenate([stacked] * (width // HEAD), axis=0)
    return jnp.where(head_blocks(width), tiled, jnp.zeros_like(tiled))


def layer_kernel(
    n_sp, n_tp,
    gain_hbm, kgain_hbm, bias_hbm, taps_hbm, ggain_hbm, gshift_hbm, hgain_hbm,
    tok_hbm, shift_hbm, extra_hbm, wcv, wcg, wk, wr, wd, we, wv, wg, wco, wao,
    out,
    gain, kgain, bias, taps, ggain, gshift, hgain,
    tok, shift, extra, cv_buf, cg_buf, k_buf, r_buf, d_buf, e_buf, v_buf, g_buf, co_buf, ao_buf,
    conv_in, extended, halo, own_map, partner_map, pair_map, maps, state,
    local_read, carried, conv_out, mix_out, conv_slots, mix_slots,
    weight_sem, halo_sem, pair_sem, map_send, map_recv, conv_send, conv_recv, mix_send, mix_recv,
):
    sp, tp = lax.axis_index("sp"), lax.axis_index("tp")
    half = tok_hbm.shape[0] // 2
    order = dict(
        gain=(gain_hbm, gain),
        tok0=(tok_hbm.at[pl.ds(0, half)], tok.at[pl.ds(0, half)]),
        tok1=(tok_hbm.at[pl.ds(half, half)], tok.at[pl.ds(half, half)]),
        k=(wk, k_buf), e=(we, e_buf), kgain=(kgain_hbm, kgain), bias=(bias_hbm, bias),
        d=(wd, d_buf), v=(wv, v_buf), shift=(shift_hbm, shift), extra=(extra_hbm, extra),
        cv=(wcv, cv_buf), cg=(wcg, cg_buf), r=(wr, r_buf), g=(wg, g_buf),
        taps=(taps_hbm, taps), ggain=(ggain_hbm, ggain), gshift=(gshift_hbm, gshift),
        hgain=(hgain_hbm, hgain), co=(wco, co_buf), ao=(wao, ao_buf),
    )
    copies = {}
    for index, (key, (source, buffer)) in enumerate(order.items()):
        copies[key] = pltpu.make_async_copy(source, buffer, weight_sem.at[index])
        copies[key].start()

    def arrive(*keys):
        for key in keys:
            copies[key].wait()

    barrier = pltpu.get_barrier_semaphore()
    for step in range(1, n_sp):
        pl.semaphore_signal(
            barrier, inc=1, device_id=(lax.rem(sp + step, n_sp), tp), device_id_type=MESH
        )
    for step in range(1, n_tp):
        pl.semaphore_signal(
            barrier, inc=1, device_id=(sp, lax.rem(tp + step, n_tp)), device_id_type=MESH
        )
    rows = tok.shape[0]
    channels = conv_in.shape[1]
    width = local_read.shape[1]
    heads = width // HEAD
    pairs = rows // PAIR
    halo_rows = halo.shape[0]
    groups = n_sp // 2
    group, parity = sp // 2, lax.rem(sp, 2)
    first_member = parity == 0
    halves = []
    arrive("gain")
    for index in range(2):
        arrive("tok" + str(index))
        x = tok[index * half:(index + 1) * half].astype(F32)
        halves.append(
            (
                x * lax.rsqrt(jnp.mean(x * x, axis=-1, keepdims=True) + NORM_EPS) * gain[...]
            ).astype(BF16)
        )
    normed = jnp.concatenate(halves, axis=0)

    def kept(x):
        return x.astype(BF16).astype(F32)

    arrive("k", "e", "kgain")
    key_all, rate = kept(dot(normed, k_buf[...])), kept(dot(normed, e_buf[...]))
    arrive("d", "v", "bias", "shift", "extra")
    slope, value = kept(dot(normed, d_buf[...])), kept(dot(normed, v_buf[...]))
    ones = jnp.where(head_blocks(width), 1.0, 0.0).astype(BF16)
    unit = key_all * kgain[...]
    unit = unit * lax.rsqrt(mm_left(unit * unit, ones) + KEY_EPS)
    erase = unit * jax.nn.sigmoid(rate)
    logits = slope + bias[...] + shift[...]
    decay = jax.nn.sigmoid(logits) * (-0.6065306597126334) + extra[...]
    row, col = iota2(PAIR, PAIR)
    same = (row // CHUNK) == (col // CHUNK)
    strict = same & (row > col)
    inclusive = same & (row >= col)
    eye = jnp.where(row == col, 1.0, 0.0)
    tri = jnp.where(inclusive, 1.0, 0.0).astype(BF16)
    cum = jnp.concatenate(
        [mm_right(tri, decay[p * PAIR:(p + 1) * PAIR], count=3) for p in range(pairs)], axis=0
    )

    def chunk_row(offset):
        return jnp.concatenate(
            [
                jnp.broadcast_to(cum[c + offset:c + offset + 1], (CHUNK, width))
                for c in range(0, rows, CHUNK)
            ],
            axis=0,
        )

    mid = chunk_row(CHUNK // 2 - 1)
    final = chunk_row(CHUNK - 1)
    before = cum - decay
    up = jnp.exp(mid - cum)
    left_unit = unit * jnp.exp(before - mid)
    right_erase = erase * up
    right_key = key_all * up
    query_unit = unit * jnp.exp(before)
    keep = jnp.exp(final - cum)
    kept_erase = erase * keep
    kept_key = key_all * keep

    units = [(h, p) for h in range(heads) for p in range(pairs)]

    def piece(values, unit_index):
        h, p = unit_index
        return values[p * PAIR:(p + 1) * PAIR, h * HEAD:(h + 1) * HEAD]

    lower, key_mix, values_of, rights = [], [], [], []
    for u in units:
        right = jnp.concatenate([piece(right_erase, u), piece(right_key, u)], axis=0)
        product = mm(piece(left_unit, u), right, "qk", NT)
        lower.append(jnp.where(strict, product[:, :PAIR], 0.0))
        key_mix.append(jnp.where(strict, product[:, PAIR:], 0.0))
        values_of.append(piece(value, u))
        rights.append(right)
    right_side = [
        -jnp.concatenate([mm(k, v, "kmv"), piece(query_unit, u)], axis=1)
        for k, v, u in zip(key_mix, values_of, units)
    ]
    first = strict & ((row // 2) == (col // 2))
    inverse = [eye - jnp.where(first, low, 0.0) for low in lower]
    size = 2
    while size < CHUNK:
        level = ((row // (2 * size)) == (col // (2 * size))) & ((row // size) > (col // size))
        inner = [mm(jnp.where(level, low, 0.0), inv, "inv") for low, inv in zip(lower, inverse)]
        inverse = [inv - mm(inv, step, "inv") for inv, step in zip(inverse, inner)]
        size *= 2
    removed = [mm(inv, rhs, "rem") for inv, rhs in zip(inverse, right_side)]
    if REFINE:
        left_over = [
            rhs - rem - mm(low, rem, "res") for rhs, rem, low in zip(right_side, removed, lower)
        ]
        removed = [
            rem + mm(inv, rest, "fix") for rem, inv, rest in zip(removed, inverse, left_over)
        ]
    eye_head = iota2(HEAD, HEAD)
    eye_head = eye_head[0] == eye_head[1]
    blocks = {}
    for h in range(heads):
        for p in range(pairs):
            index = h * pairs + p
            ke, kk = piece(kept_erase, (h, p)), piece(kept_key, (h, p))
            for half in range(PAIR // CHUNK):
                span = slice(half * CHUNK, (half + 1) * CHUNK)
                start = p * PAIR + half * CHUNK
                from_removed = mm(removed[index][span], ke[span], "keep", TN)
                base = from_removed[:HEAD] + mm(values_of[index][span], kk[span], "keep", TN)
                last = jnp.exp(final[start:start + 1, h * HEAD:(h + 1) * HEAD])
                trans = from_removed[HEAD:] + jnp.where(eye_head, last, 0.0)
                blocks[h, start // CHUNK] = (base, trans)
    priors = {}
    totals = [None] * heads
    for chunk in range(rows // CHUNK):
        for h in range(heads):
            base, trans = blocks[h, chunk]
            priors[h, chunk] = totals[h]
            if totals[h] is None:
                totals[h] = jnp.concatenate([base, trans], axis=0)
            else:
                moved = mm(totals[h], trans, "state")
                totals[h] = jnp.concatenate([moved[:HEAD] + base, moved[HEAD:]], axis=0)
    own_total = jnp.concatenate(totals, axis=1).astype(WIRE)
    own_map[...] = own_total

    pl.semaphore_wait(barrier, n_sp + n_tp - 2)
    pair_copy = pltpu.make_async_remote_copy(
        src_ref=own_map, dst_ref=partner_map, send_sem=pair_sem.at[0], recv_sem=pair_sem.at[1],
        device_id=(sp + 1 - 2 * parity, tp), device_id_type=MESH,
    )
    pair_copy.start()

    arrive("cv", "cg")
    both = jnp.concatenate([cv_buf[...], cg_buf[...]], axis=1)
    pair = kept(jnp.concatenate([dot(part, both) for part in halves], axis=0))
    conv_rows = (pair[:, :channels] * jax.nn.sigmoid(pair[:, channels:])).astype(BF16)
    conv_in[...] = conv_rows
    halo_copy = pltpu.make_async_remote_copy(
        src_ref=conv_in.at[pl.ds(rows - halo_rows, halo_rows)], dst_ref=halo,
        send_sem=halo_sem.at[0], recv_sem=halo_sem.at[1],
        device_id=(sp + 1, tp), device_id_type=MESH,
    )
    has_next = sp + 1 < n_sp

    @pl.when(has_next)
    def _():
        halo_copy.start()

    extended[halo_rows:, :] = conv_rows.astype(F32)

    def chain(carry, block):
        trans = block_diagonal(block[HEAD:], width)
        return mm(carry, trans, "enter")

    arrive("r", "g", "hgain")
    receptance, gate = kept(dot(normed, r_buf[...])), kept(dot(normed, g_buf[...]))
    gate = jax.nn.sigmoid(gate) * hgain[...]
    left_read = receptance * jnp.exp(cum - mid)
    query_read = receptance * jnp.exp(cum)

    pair_copy.wait()
    mine, theirs = own_total.astype(F32), partner_map[...].astype(F32)
    early = jnp.where(first_member, mine, theirs)
    late = jnp.where(first_member, theirs, mine)
    joined = chain(early, late)
    pair_map[:HEAD] = (joined[:HEAD] + late[:HEAD]).astype(WIRE)
    pair_map[HEAD:] = joined[HEAD:].astype(WIRE)

    def map_copy(ahead):
        return pltpu.make_async_remote_copy(
            src_ref=pair_map, dst_ref=maps.at[ahead],
            send_sem=map_send.at[ahead], recv_sem=map_recv.at[ahead],
            device_id=(sp + 2 * ahead, tp), device_id_type=MESH,
        )

    for ahead in range(1, groups):
        @pl.when(group + ahead < groups)
        def _():
            map_copy(ahead).start()

    @pl.when(sp > 0)
    def _():
        halo_copy.wait_recv()
        extended[:halo_rows, :] = halo[...].astype(F32)

    @pl.when(sp == 0)
    def _():
        extended[:halo_rows, :] = jnp.zeros((halo_rows, channels), F32)

    arrive("taps", "ggain", "gshift")
    tap_count = taps.shape[0]
    total = jnp.zeros((rows, channels), F32)
    for offset in range(tap_count):
        begin = halo_rows - tap_count + 1 + offset
        total = total + taps[offset:offset + 1, :] * extended[begin:begin + rows, :]
    means = jnp.where(head_blocks(channels), 1.0 / HEAD, 0.0).astype(BF16)
    centred = total - mm_left(total, means)
    scaled = centred * lax.rsqrt(mm_left(centred * centred, means) + GROUP_EPS)
    conv_out[...] = jax.nn.silu(scaled * ggain[...] + gshift[...]).astype(BF16)

    span = rows // n_tp

    def spread(source, slots, send, recv):
        started = []
        for step in range(1, n_tp):
            target = lax.rem(tp + step, n_tp)
            begin = pl.multiple_of(target * span, span)
            copy = pltpu.make_async_remote_copy(
                src_ref=source.at[pl.ds(begin, span)], dst_ref=slots.at[step],
                send_sem=send.at[step], recv_sem=recv.at[step],
                device_id=(sp, target), device_id_type=MESH,
            )
            copy.start()
            started.append(copy)
        return started

    conv_copies = spread(conv_out, conv_slots, conv_send, conv_recv)

    zeros = jnp.zeros((PAIR, HEAD), F32)
    for index, u in enumerate(units):
        h, p = u
        product = mm(piece(left_read, u), rights[index], "qk", NT)
        mix = jnp.concatenate(
            [
                jnp.where(inclusive, product[:, :PAIR], 0.0),
                jnp.where(inclusive, product[:, PAIR:], 0.0),
            ],
            axis=1,
        )
        stacked = jnp.concatenate(
            [removed[index], jnp.concatenate([values_of[index], zeros], axis=1)], axis=0
        )
        readout = mm(mix, stacked, "read") + jnp.concatenate(
            [zeros, piece(query_read, u)], axis=1
        )
        for half in range(PAIR // CHUNK):
            start = p * PAIR + half * CHUNK
            lanes = slice(h * HEAD, (h + 1) * HEAD)
            read = readout[half * CHUNK:(half + 1) * CHUNK]
            prior = priors[h, start // CHUNK]
            if prior is not None:
                read = jnp.concatenate(
                    [read[:, :HEAD], jnp.zeros((CHUNK, HEAD), F32)], axis=1
                ) + mm(read[:, HEAD:], prior, "carry", NT)
            local_read[start:start + CHUNK, lanes] = read[:, :HEAD]
            carried[start:start + CHUNK, lanes] = read[:, HEAD:]

    own = pl.multiple_of(tp * span, span)

    def gather(result, source, slots, arriving, weight, depth):
        result = result + dot(
            source[pl.ds(own, span)], weight[pl.ds(pl.multiple_of(tp * depth, depth), depth)]
        )
        for step in range(1, n_tp):
            arriving[step - 1].wait_recv()
            begin = lax.rem(tp - step + n_tp, n_tp) * depth
            result = result + dot(
                slots[step], weight[pl.ds(pl.multiple_of(begin, depth), depth)]
            )
        return result

    arrive("co")
    result = gather(
        jnp.zeros(out.shape, F32), conv_out, conv_slots, conv_copies, co_buf, channels
    )

    state[...] = jnp.zeros_like(state)
    for ahead in range(groups - 1, 0, -1):
        @pl.when(group >= ahead)
        def _():
            map_copy(ahead).wait_recv()
            block = maps[ahead].astype(F32)
            state[...] = chain(state[...], block) + block[:HEAD]

    behind = chain(state[...], early) + early[:HEAD]
    entering = jnp.where(first_member, state[...], behind)
    readout = local_read[...] + mm(carried[...], block_diagonal(entering, width), "enter", NT)
    head_means = jnp.where(head_blocks(width), 1.0 / HEAD, 0.0).astype(BF16)
    centred = readout - mm_left(readout, head_means)
    scaled = centred * lax.rsqrt(mm_left(centred * centred, head_means) + HEAD_EPS)
    mix_out[...] = (scaled * gate).astype(BF16)
    mix_copies = spread(mix_out, mix_slots, mix_send, mix_recv)
    arrive("ao")
    result = gather(result, mix_out, mix_slots, mix_copies, ao_buf, width)
    out[...] = result.astype(BF16)
    for copy in conv_copies + mix_copies:
        copy.wait_send()

    @pl.when(has_next)
    def _():
        halo_copy.wait_send()

    for ahead in range(1, groups):
        @pl.when(group + ahead < groups)
        def _():
            map_copy(ahead).wait_send()


def local(
    n_sp, n_tp,
    tokens, input_norm_gain, convolution_value_weight, convolution_gate_weight,
    depthwise_taps_weight, convolution_group_gain, convolution_group_shift,
    receptance_weight, key_weight, value_weight, decay_weight, correction_rate_weight,
    output_gate_weight, key_prenorm_gain, decay_offset_bias, position_decay_shift,
    extra_log_decay, head_norm_gain, convolution_output_weight, attention_output_weight,
):
    rows, model = tokens.shape
    channels = convolution_value_weight.shape[1]
    width = key_weight.shape[1]
    vmem = pl.BlockSpec(memory_space=pltpu.VMEM)
    anywhere = pl.BlockSpec(memory_space=pl.ANY)

    def line(values):
        return values.reshape(1, -1)

    smalls = (
        line(input_norm_gain), line(key_prenorm_gain), line(decay_offset_bias),
        depthwise_taps_weight, line(convolution_group_gain), line(convolution_group_shift),
        line(head_norm_gain),
    )
    weights = (
        convolution_value_weight, convolution_gate_weight, key_weight, receptance_weight,
        decay_weight, correction_rate_weight, value_weight, output_gate_weight,
        convolution_output_weight, attention_output_weight,
    )
    span = rows // n_tp
    halo_rows = -(-(depthwise_taps_weight.shape[0] - 1) // 16) * 16
    groups = n_sp // 2
    dma = pltpu.SemaphoreType.DMA
    map_shape = (2 * HEAD, width)
    return pl.pallas_call(
        functools.partial(layer_kernel, n_sp, n_tp),
        name="layer",
        out_shape=pltpu.VMEM((span, model), BF16),
        in_specs=[anywhere] * 20,
        out_specs=vmem,
        scratch_shapes=[pltpu.VMEM(small.shape, F32) for small in smalls]
        + [
            pltpu.VMEM(tokens.shape, BF16),
            pltpu.VMEM(position_decay_shift.shape, F32),
            pltpu.VMEM(extra_log_decay.shape, F32),
        ]
        + [pltpu.VMEM(weight.shape, BF16) for weight in weights]
        + [
            pltpu.VMEM((rows, channels), BF16),
            pltpu.VMEM((halo_rows + rows, channels), F32),
            pltpu.VMEM((halo_rows, channels), BF16),
            pltpu.VMEM(map_shape, WIRE),
            pltpu.VMEM(map_shape, WIRE),
            pltpu.VMEM(map_shape, WIRE),
            pltpu.VMEM((groups,) + map_shape, WIRE),
            pltpu.VMEM((HEAD, width), F32),
            pltpu.VMEM((rows, width), F32),
            pltpu.VMEM((rows, width), F32),
            pltpu.VMEM((rows, channels), BF16),
            pltpu.VMEM((rows, width), BF16),
            pltpu.VMEM((n_tp, span, channels), BF16),
            pltpu.VMEM((n_tp, span, width), BF16),
            dma((21,)), dma((2,)), dma((2,)), dma((groups,)), dma((groups,)),
            dma((n_tp,)), dma((n_tp,)), dma((n_tp,)), dma((n_tp,)),
        ],
        compiler_params=pltpu.CompilerParams(
            collective_id=0, has_side_effects=True, vmem_limit_bytes=VMEM_LIMIT
        ),
    )(
        *smalls, tokens, position_decay_shift, extra_log_decay, *weights,
    )


def solution(mesh):
    in_specs = (
        P("sp", None),
        P(),
        P(None, "tp"),
        P(None, "tp"),
        P(None, "tp"),
        P("tp"),
        P("tp"),
        P(None, "tp"),
        P(None, "tp"),
        P(None, "tp"),
        P(None, "tp"),
        P(None, "tp"),
        P(None, "tp"),
        P("tp"),
        P("tp"),
        P("sp", "tp"),
        P("sp", "tp"),
        P("tp"),
        P(),
        P(),
    )
    body = functools.partial(local, mesh.shape["sp"], mesh.shape["tp"])
    return jax.shard_map(
        body, mesh=mesh, in_specs=in_specs, out_specs=P(("sp", "tp"), None), check_vma=False
    )
```

```python
import functools

import jax
import jax.numpy as jnp
from jax import lax
from jax.experimental import pallas as pl
from jax.experimental.pallas import tpu as pltpu
from jax.sharding import PartitionSpec as P

HEAD = 64
CHUNK = 64
TOKEN_PARTS = 4
PAIR = 128

NORM_EPS = 1e-06
GROUP_EPS = 1e-05
HEAD_EPS = 0.00064
KEY_EPS = 1e-06
MESH = pl.DeviceIdType.MESH
WIRE = jnp.bfloat16
VMEM_LIMIT = 60 * 1024 * 1024
F32 = jnp.float32
BF16 = jnp.bfloat16

NN = (((1,), (0,)), ((), ()))
NT = (((1,), (1,)), ((), ()))
TN = (((0,), (0,)), ((), ()))


def parts(x, count):
    out = []
    for _ in range(count - 1):
        piece = x.astype(BF16)
        out.append(piece)
        x = x - piece.astype(F32)
    out.append(x.astype(BF16))
    return out


def dot(a, b, dims=NN):
    return lax.dot_general(a, b, dims, preferred_element_type=F32)


def mm_left(a, b, dims=NN, count=2):
    pieces = [dot(piece, b, dims) for piece in parts(a, count)]
    return functools.reduce(jnp.add, pieces)


def split(x):
    high = x.astype(BF16)
    return high, (x - high.astype(F32)).astype(BF16)


def concat(pieces, axis=0):
    return jnp.concatenate(pieces, axis=axis)


def iota2(rows, cols):
    return (
        lax.broadcasted_iota(jnp.int32, (rows, cols), 0),
        lax.broadcasted_iota(jnp.int32, (rows, cols), 1),
    )


def head_blocks(width):
    row, col = iota2(width, width)
    return (row // HEAD) == (col // HEAD)


def own_head(shape):
    row, col = iota2(*shape)
    return (row // HEAD) == ((col % PAIR) // HEAD)


def diagonal(x):
    lane = lax.broadcasted_iota(jnp.int32, x.shape, 1)
    zero = jnp.zeros_like(x)
    return concat([jnp.where(lane < HEAD, x, zero), jnp.where(lane < HEAD, zero, x)])


def spread_pair(x):
    return concat([diagonal(x[:, :PAIR]), diagonal(x[:, PAIR:])], axis=1)


def compose(later, earlier):
    high, low = split(later[:, PAIR:])
    early_high, early_low = split(earlier)
    both = dot(concat([high, low]), spread_pair(early_high))
    out = both[:HEAD] + both[HEAD:] + dot(high, spread_pair(early_low))
    return concat([out[:, :PAIR] + later[:, :PAIR], out[:, PAIR:]], axis=1)


def layer_kernel(
    n_sp, n_tp,
    gain_hbm, kgain_hbm, bias_hbm, taps_hbm, ggain_hbm, gshift_hbm, hgain_hbm,
    tok_hbm, shift_hbm, extra_hbm, wcv, wcg, wk, wr, wd, we, wv, wg, wco, wao,
    out,
    gain, kgain, bias, taps, ggain, gshift, hgain,
    tok, shift, extra, cv_buf, cg_buf, k_buf, r_buf, d_buf, e_buf, v_buf, g_buf, co_buf, ao_buf,
    conv_in, extended, halo, own_map, partner_map, pair_map, maps, windows, state, reach,
    local_read, carried, conv_out, mix_out, conv_slots, mix_slots,
    weight_sem, halo_sem, pair_sem, map_send, map_recv, conv_send, conv_recv, mix_send, mix_recv,
):
    sp, tp = lax.axis_index("sp"), lax.axis_index("tp")
    part = tok_hbm.shape[0] // TOKEN_PARTS
    order = dict(gain=(gain_hbm, gain))
    for index in range(TOKEN_PARTS):
        span = pl.ds(index * part, part)
        order["tok" + str(index)] = (tok_hbm.at[span], tok.at[span])
    order.update(
        k=(wk, k_buf), e=(we, e_buf), kgain=(kgain_hbm, kgain),
        d=(wd, d_buf), v=(wv, v_buf), bias=(bias_hbm, bias),
        shift=(shift_hbm, shift), extra=(extra_hbm, extra),
        cv=(wcv, cv_buf), cg=(wcg, cg_buf), r=(wr, r_buf), g=(wg, g_buf),
        taps=(taps_hbm, taps), ggain=(ggain_hbm, ggain), gshift=(gshift_hbm, gshift),
        hgain=(hgain_hbm, hgain), co=(wco, co_buf), ao=(wao, ao_buf),
    )
    copies = {}
    for index, (key, (source, buffer)) in enumerate(order.items()):
        copies[key] = pltpu.make_async_copy(source, buffer, weight_sem.at[index])

    def begin(*keys):
        for key in keys:
            copies[key].start()

    def arrive(*keys):
        for key in keys:
            copies[key].wait()

    token_keys = ["tok" + str(index) for index in range(TOKEN_PARTS)]
    begin("gain", *token_keys, "k", "e", "kgain", "d", "v", "bias", "shift", "extra")
    barrier = pltpu.get_barrier_semaphore()
    for step in range(1, n_sp):
        pl.semaphore_signal(
            barrier, inc=1, device_id=(lax.rem(sp + step, n_sp), tp), device_id_type=MESH
        )
    for step in range(1, n_tp):
        pl.semaphore_signal(
            barrier, inc=1, device_id=(sp, lax.rem(tp + step, n_tp)), device_id_type=MESH
        )
    rows = tok.shape[0]
    channels = conv_in.shape[1]
    width = local_read.shape[1]
    heads = width // HEAD
    pairs = rows // PAIR
    halo_rows = halo.shape[0]
    groups = n_sp // 2
    group, parity = sp // 2, lax.rem(sp, 2)
    first_member = parity == 0
    quarters = []
    arrive("gain")
    for index, key in enumerate(token_keys):
        arrive(key)
        x = tok[index * part:(index + 1) * part].astype(F32)
        quarters.append(
            (
                x * lax.rsqrt(jnp.mean(x * x, axis=-1, keepdims=True) + NORM_EPS) * gain[...]
            ).astype(BF16)
        )
    begin("cv", "cg", "r", "g", "taps", "ggain", "gshift", "hgain")
    middle_part = TOKEN_PARTS // 2
    halves = [concat(quarters[:middle_part]), concat(quarters[middle_part:])]
    normed = concat(halves)

    def kept(x):
        return x.astype(BF16).astype(F32)

    arrive("k", "e", "kgain")
    key_all, rate = kept(dot(normed, k_buf[...])), kept(dot(normed, e_buf[...]))
    arrive("d", "v", "bias", "shift", "extra")
    begin("co", "ao")
    slope = kept(dot(normed, d_buf[...]))
    value = dot(normed, v_buf[...]).astype(BF16)
    same_head = head_blocks(width)
    ones = jnp.where(same_head, 1.0, 0.0).astype(BF16)
    row, col = iota2(width, width)
    centre = (jnp.where(row == col, 1.0, 0.0) - jnp.where(same_head, 1.0 / HEAD, 0.0)).astype(BF16)
    unit = key_all * kgain[...]
    unit = unit * lax.rsqrt(dot((unit * unit).astype(BF16), ones) + KEY_EPS)
    erase = -(unit * jax.nn.sigmoid(rate))
    value_high, value_low = split(dot(value, centre))
    logits = slope + bias[...] + shift[...]
    decay = jax.nn.sigmoid(logits) * (-0.6065306597126334) + extra[...]
    row, col = iota2(PAIR, 2 * PAIR)
    col = col % PAIR
    tri = jnp.where(((row // CHUNK) == (col // CHUNK)) & (row >= col), 1.0, 0.0).astype(BF16)
    cum = concat(
        [dot(tri, concat(split(decay[p:p + PAIR]))) for p in range(0, rows, PAIR)]
    )
    chunks = rows // CHUNK
    groups_of = width // PAIR

    def by_chunk(row_of):
        return concat(
            [jnp.broadcast_to(row_of(c), (CHUNK, width)) for c in range(0, rows, CHUNK)]
        )

    def middle(c):
        return cum[c + CHUNK // 2 - 1:c + CHUNK // 2]

    def last(c):
        return cum[c + CHUNK - 1:c + CHUNK]

    mid = by_chunk(middle)
    from_start = by_chunk(lambda c: jnp.exp(middle(c)))
    to_end = by_chunk(lambda c: jnp.exp(last(c) - middle(c)))
    up = jnp.exp(mid - cum)
    left_unit = unit * jnp.exp(cum - decay - mid)
    query_unit = (left_unit * from_start).astype(BF16)
    left_unit = left_unit.astype(BF16)
    right_erase, right_key = erase * up, key_all * up
    kept_erase, kept_key = (right_erase * to_end).astype(BF16), (right_key * to_end).astype(BF16)
    right_erase, right_key = right_erase.astype(BF16), right_key.astype(BF16)
    units = [(c, g) for c in range(chunks) for g in range(groups_of)]

    def piece(values, unit_index):
        c, g = unit_index
        return values[c * CHUNK:(c + 1) * CHUNK, g * PAIR:(g + 1) * PAIR]

    row, col = iota2(CHUNK, PAIR)
    col = col % CHUNK
    strict, inclusive = row > col, row >= col
    eye = jnp.where(row == col, 1.0, 0.0)
    rights = [
        concat([diagonal(piece(right_erase, u)), diagonal(piece(right_key, u))]) for u in units
    ]
    products = [dot(piece(left_unit, u), right, NT) for u, right in zip(units, rights)]
    lower = [jnp.where(strict, product[:, :PAIR], 0.0) for product in products]
    mixes = [jnp.where(strict, product[:, PAIR:], 0.0).astype(BF16) for product in products]
    value_diagonals = [
        concat([diagonal(piece(value_high, u)), diagonal(piece(value_low, u))]) for u in units
    ]
    mixed = [
        dot(concat([mix, mix], axis=1), both) for mix, both in zip(mixes, value_diagonals)
    ]
    first = strict & ((row // 2) == (col // 2))
    inverse = [eye + jnp.where(first, low, 0.0) for low in lower]
    size = 2
    while size < CHUNK:
        level = ((row // (2 * size)) == (col // (2 * size))) & ((row // size) > (col // size))
        narrow = [inv.astype(BF16) for inv in inverse]
        inner = [
            dot(jnp.where(level, low, 0.0).astype(BF16), diagonal(inv))
            for low, inv in zip(lower, narrow)
        ]
        inverse = [
            inv + dot(left, diagonal(step.astype(BF16)))
            for inv, left, step in zip(inverse, narrow, inner)
        ]
        size *= 2
    solved = [
        dot(
            inv.astype(BF16),
            concat([diagonal(mix.astype(BF16)), diagonal(piece(query_unit, u))], axis=1),
        ).astype(BF16)
        for inv, mix, u in zip(inverse, mixed, units)
    ]
    nothing = jnp.zeros((CHUNK, PAIR), BF16)
    lane = lax.broadcasted_iota(jnp.int32, (HEAD, 2 * PAIR), 1)
    first_head = (lane % PAIR) < HEAD
    blocks = {}
    for index, u in enumerate(units):
        c, g = u
        left = concat([piece(kept_erase, u), piece(kept_key, u), piece(kept_key, u)])
        right = concat(
            [
                solved[index],
                concat([piece(value_high, u), nothing], axis=1),
                concat([piece(value_low, u), nothing], axis=1),
            ]
        )
        product = dot(left, right, TN)
        product = jnp.where(first_head, product[:HEAD], product[HEAD:])
        stay = jnp.exp(last(c * CHUNK)[:, g * PAIR:(g + 1) * PAIR])
        blocks[u] = concat([product[:, :PAIR], product[:, PAIR:] + eye * stay], axis=1)
    spans = {}
    for c in range(chunks):
        for g in range(groups_of):
            spans[c, c + 1, g] = blocks[c, g]
    size = 1
    while size < chunks:
        for c in range(0, chunks, 2 * size):
            for g in range(groups_of):
                spans[c, c + 2 * size, g] = compose(
                    spans[c + size, c + 2 * size, g], spans[c, c + size, g]
                )
        size *= 2
    totals = [spans[0, chunks, g] for g in range(groups_of)]
    own_total = concat(
        [
            concat([totals[g][:, :PAIR] for g in range(groups_of)], axis=1),
            concat([totals[g][:, PAIR:] for g in range(groups_of)], axis=1),
        ]
    ).astype(WIRE)
    own_map[...] = own_total

    pl.semaphore_wait(barrier, n_sp + n_tp - 2)
    pair_copy = pltpu.make_async_remote_copy(
        src_ref=own_map, dst_ref=partner_map, send_sem=pair_sem.at[0], recv_sem=pair_sem.at[1],
        device_id=(sp + 1 - 2 * parity, tp), device_id_type=MESH,
    )
    pair_copy.start()

    arrive("cv", "cg")
    both = concat([cv_buf[...], cg_buf[...]], axis=1)
    conv_pair = kept(concat([dot(part, both) for part in halves]))
    conv_rows = (
        conv_pair[:, :channels] * jax.nn.sigmoid(conv_pair[:, channels:])
    ).astype(BF16)
    conv_in[...] = conv_rows
    halo_copy = pltpu.make_async_remote_copy(
        src_ref=conv_in.at[pl.ds(rows - halo_rows, halo_rows)], dst_ref=halo,
        send_sem=halo_sem.at[0], recv_sem=halo_sem.at[1],
        device_id=(sp + 1, tp), device_id_type=MESH,
    )
    has_next = sp + 1 < n_sp

    @pl.when(has_next)
    def _():
        halo_copy.start()

    extended[halo_rows:, :] = conv_rows.astype(F32)

    arrive("r", "g", "hgain")
    receptance, gate = kept(dot(normed, r_buf[...])), kept(dot(normed, g_buf[...]))
    left_read = receptance * jnp.exp(cum - mid)
    query_read = left_read * from_start
    left_read = left_read.astype(BF16)
    gate = jax.nn.sigmoid(gate) * hgain[...]
    zeros = jnp.zeros((PAIR, PAIR), BF16)
    products = [dot(piece(left_read, u), right, NT) for u, right in zip(units, rights)]
    reads = []
    for product, end, both, u in zip(products, solved, value_diagonals, units):
        keys = jnp.where(inclusive, product[:, PAIR:], 0.0).astype(BF16)
        mix = concat(
            [jnp.where(inclusive, product[:, :PAIR], 0.0).astype(BF16), keys, keys], axis=1
        )
        stacked = concat(
            [spread_pair(end), concat([both, concat([zeros, zeros])], axis=1)]
        )
        reads.append(dot(mix, stacked))
    priors = {}
    for c in range(1, chunks):
        start, size = 0, chunks // 2
        while start < c:
            while start + size > c:
                size //= 2
            for g in range(groups_of):
                block = spans[start, start + size, g]
                priors[c, g] = block if start == 0 else compose(block, priors[c, g])
            start += size
    for index, u in enumerate(units):
        c, g = u
        near, far = reads[index][:, :PAIR], reads[index][:, PAIR:] + piece(query_read, u)
        if c > 0:
            moved = dot(far.astype(BF16), spread_pair(priors[u].astype(BF16)))
            near, far = near + moved[:, :PAIR], moved[:, PAIR:]
        span = slice(c * CHUNK, (c + 1) * CHUNK)
        lanes = slice(g * PAIR, (g + 1) * PAIR)
        local_read[span, lanes] = near
        carried[span, lanes] = far.astype(BF16)

    def by_pair(x):
        return [x[:, g * PAIR:(g + 1) * PAIR] for g in range(groups_of)]

    def chain(held, move):
        out = []
        for state_part, move_part in zip(by_pair(held), by_pair(move)):
            right = concat([diagonal(piece_of) for piece_of in split(state_part)])
            out.append(dot(concat([move_part, move_part], axis=1), right))
        return concat(out, axis=1)

    pair_copy.wait()
    mine, theirs = own_total.astype(F32), partner_map[...].astype(F32)
    early = jnp.where(first_member, mine, theirs).astype(WIRE)
    late = jnp.where(first_member, theirs, mine).astype(WIRE)
    joined = [
        dot(move, spread_pair(concat([add, keep], axis=1)))
        for move, add, keep in zip(by_pair(late[HEAD:]), by_pair(early[:HEAD]), by_pair(early[HEAD:]))
    ]
    pair_map[:HEAD] = (
        concat([part[:, :PAIR] for part in joined], axis=1) + late[:HEAD].astype(F32)
    ).astype(WIRE)
    pair_map[HEAD:] = concat([part[:, PAIR:] for part in joined], axis=1).astype(WIRE)

    hops = []
    while 2 ** len(hops) < groups:
        hops.append(2 ** len(hops))

    def hop(source, k, side):
        span_of = pl.ds(side * HEAD, HEAD)
        return pltpu.make_async_remote_copy(
            src_ref=source.at[span_of], dst_ref=maps.at[k, span_of],
            send_sem=map_send.at[2 * k + side], recv_sem=map_recv.at[2 * k + side],
            device_id=(sp + 2 * hops[k], tp), device_id_type=MESH,
        )

    sends = []
    for k, ahead in enumerate(hops):
        reached = group + ahead < groups
        if k == 0:
            sends.append((k, reached, pair_map, 0))
            sends.append((k, reached & (group >= 1), pair_map, 1))
        else:
            sends.append((0, group == 0, pair_map, 0, k))
            sends.append((k, reached & (group >= 1), windows.at[k], 0))
            if 2 * ahead < groups:
                sends.append((k, reached & (group >= ahead), windows.at[k], 1))

    def send_step(step):
        for when, allowed, source, side, *target in sends:
            if when == step:
                @pl.when(allowed)
                def _():
                    hop(source, target[0] if target else step, side).start()

    if hops:
        send_step(0)

    @pl.when(sp > 0)
    def _():
        halo_copy.wait_recv()
        extended[:halo_rows, :] = halo[...].astype(F32)

    @pl.when(sp == 0)
    def _():
        extended[:halo_rows, :] = jnp.zeros((halo_rows, channels), F32)

    arrive("taps", "ggain", "gshift")
    tap_count = taps.shape[0]
    total = jnp.zeros((rows, channels), F32)
    for offset in range(tap_count):
        begin = halo_rows - tap_count + 1 + offset
        total = total + taps[offset:offset + 1, :] * extended[begin:begin + rows, :]
    means = jnp.where(head_blocks(channels), 1.0 / HEAD, 0.0).astype(BF16)
    centred = total - mm_left(total, means)
    scaled = centred * lax.rsqrt(mm_left(centred * centred, means) + GROUP_EPS)
    conv_out[...] = jax.nn.silu(scaled * ggain[...] + gshift[...]).astype(BF16)

    span = rows // n_tp

    def spread(source, slots, send, recv):
        started = []
        for step in range(1, n_tp):
            target = lax.rem(tp + step, n_tp)
            begin = pl.multiple_of(target * span, span)
            copy = pltpu.make_async_remote_copy(
                src_ref=source.at[pl.ds(begin, span)], dst_ref=slots.at[step],
                send_sem=send.at[step], recv_sem=recv.at[step],
                device_id=(sp, target), device_id_type=MESH,
            )
            copy.start()
            started.append(copy)
        return started

    conv_copies = spread(conv_out, conv_slots, conv_send, conv_recv)

    own = pl.multiple_of(tp * span, span)

    def gather(result, source, slots, arriving, weight, depth):
        result = result + dot(
            source[pl.ds(own, span)], weight[pl.ds(pl.multiple_of(tp * depth, depth), depth)]
        )
        for step in range(1, n_tp):
            arriving[step - 1].wait_recv()
            begin = lax.rem(tp - step + n_tp, n_tp) * depth
            result = result + dot(
                slots[step], weight[pl.ds(pl.multiple_of(begin, depth), depth)]
            )
        return result

    state[...] = jnp.zeros_like(state)
    for k, ahead in enumerate(hops):
        @pl.when(group >= ahead)
        def _():
            hop(pair_map, k, 0).wait_recv()
            arrived = maps[k, :HEAD].astype(F32)
            state[...] = arrived if k == 0 else chain(arrived, reach[...]) + state[...]

        if 2 * ahead < groups:
            @pl.when(group >= 2 * ahead)
            def _():
                hop(pair_map, k, 1).wait_recv()
                further = maps[k, HEAD:]
                if k > 0:
                    further = chain(further.astype(F32), reach[...]).astype(WIRE)
                reach[...] = further

            following = 2 * ahead

            @pl.when((group >= 1) & (group + following < groups))
            def _():
                windows[k + 1, :HEAD] = (
                    chain(state[...], pair_map[HEAD:]) + pair_map[:HEAD].astype(F32)
                ).astype(WIRE)

            if 2 * following < groups:
                @pl.when((group >= following) & (group + following < groups))
                def _():
                    windows[k + 1, HEAD:] = chain(
                        reach[...].astype(F32), pair_map[HEAD:]
                    ).astype(WIRE)

            send_step(k + 1)

    behind = chain(state[...], early[HEAD:]) + early[:HEAD].astype(F32)
    entering = jnp.where(first_member, state[...], behind).astype(BF16)
    centred = local_read[...] + concat(
        [
            dot(carried[:, g * PAIR:(g + 1) * PAIR], diagonal(part))
            for g, part in enumerate(by_pair(entering))
        ],
        axis=1,
    )
    head_means = jnp.where(same_head, 1.0 / HEAD, 0.0).astype(BF16)
    scaled = centred * lax.rsqrt(dot((centred * centred).astype(BF16), head_means) + HEAD_EPS)
    mix_out[...] = (scaled * gate).astype(BF16)
    mix_copies = spread(mix_out, mix_slots, mix_send, mix_recv)
    arrive("co")
    result = gather(
        jnp.zeros(out.shape, F32), conv_out, conv_slots, conv_copies, co_buf, channels
    )

    arrive("ao")
    result = gather(result, mix_out, mix_slots, mix_copies, ao_buf, width)
    out[...] = result.astype(BF16)
    for copy in conv_copies + mix_copies:
        copy.wait_send()

    @pl.when(has_next)
    def _():
        halo_copy.wait_send()

    for when, allowed, source, side, *target in sends:
        @pl.when(allowed)
        def _():
            hop(source, target[0] if target else when, side).wait_send()


def local(
    n_sp, n_tp,
    tokens, input_norm_gain, convolution_value_weight, convolution_gate_weight,
    depthwise_taps_weight, convolution_group_gain, convolution_group_shift,
    receptance_weight, key_weight, value_weight, decay_weight, correction_rate_weight,
    output_gate_weight, key_prenorm_gain, decay_offset_bias, position_decay_shift,
    extra_log_decay, head_norm_gain, convolution_output_weight, attention_output_weight,
):
    rows, model = tokens.shape
    channels = convolution_value_weight.shape[1]
    width = key_weight.shape[1]
    vmem = pl.BlockSpec(memory_space=pltpu.VMEM)
    anywhere = pl.BlockSpec(memory_space=pl.ANY)

    def line(values):
        return values.reshape(1, -1)

    smalls = (
        line(input_norm_gain), line(key_prenorm_gain), line(decay_offset_bias),
        depthwise_taps_weight, line(convolution_group_gain), line(convolution_group_shift),
        line(head_norm_gain),
    )
    weights = (
        convolution_value_weight, convolution_gate_weight, key_weight, receptance_weight,
        decay_weight, correction_rate_weight, value_weight, output_gate_weight,
        convolution_output_weight, attention_output_weight,
    )
    span = rows // n_tp
    halo_rows = -(-(depthwise_taps_weight.shape[0] - 1) // 16) * 16
    hop_count = max(1, (n_sp // 2 - 1).bit_length())
    dma = pltpu.SemaphoreType.DMA
    map_shape = (2 * HEAD, width)
    return pl.pallas_call(
        functools.partial(layer_kernel, n_sp, n_tp),
        name="layer",
        out_shape=pltpu.VMEM((span, model), BF16),
        in_specs=[anywhere] * 20,
        out_specs=vmem,
        scratch_shapes=[pltpu.VMEM(small.shape, F32) for small in smalls]
        + [
            pltpu.VMEM(tokens.shape, BF16),
            pltpu.VMEM(position_decay_shift.shape, F32),
            pltpu.VMEM(extra_log_decay.shape, F32),
        ]
        + [pltpu.VMEM(weight.shape, BF16) for weight in weights]
        + [
            pltpu.VMEM((rows, channels), BF16),
            pltpu.VMEM((halo_rows + rows, channels), F32),
            pltpu.VMEM((halo_rows, channels), BF16),
            pltpu.VMEM(map_shape, WIRE),
            pltpu.VMEM(map_shape, WIRE),
            pltpu.VMEM(map_shape, WIRE),
            pltpu.VMEM((hop_count,) + map_shape, WIRE),
            pltpu.VMEM((hop_count,) + map_shape, WIRE),
            pltpu.VMEM((HEAD, width), F32),
            pltpu.VMEM((HEAD, width), WIRE),
            pltpu.VMEM((rows, width), F32),
            pltpu.VMEM((rows, width), BF16),
            pltpu.VMEM((rows, channels), BF16),
            pltpu.VMEM((rows, width), BF16),
            pltpu.VMEM((n_tp, span, channels), BF16),
            pltpu.VMEM((n_tp, span, width), BF16),
            dma((24,)), dma((2,)), dma((2,)), dma((2 * hop_count,)), dma((2 * hop_count,)),
            dma((n_tp,)), dma((n_tp,)), dma((n_tp,)), dma((n_tp,)),
        ],
        compiler_params=pltpu.CompilerParams(
            collective_id=0, has_side_effects=True, vmem_limit_bytes=VMEM_LIMIT
        ),
    )(
        *smalls, tokens, position_decay_shift, extra_log_decay, *weights,
    )


def solution(mesh):
    in_specs = (
        P("sp", None),
        P(),
        P(None, "tp"),
        P(None, "tp"),
        P(None, "tp"),
        P("tp"),
        P("tp"),
        P(None, "tp"),
        P(None, "tp"),
        P(None, "tp"),
        P(None, "tp"),
        P(None, "tp"),
        P(None, "tp"),
        P("tp"),
        P("tp"),
        P("sp", "tp"),
        P("sp", "tp"),
        P("tp"),
        P(),
        P(),
    )
    body = functools.partial(local, mesh.shape["sp"], mesh.shape["tp"])
    return jax.shard_map(
        body, mesh=mesh, in_specs=in_specs, out_specs=P(("sp", "tp"), None), check_vma=False
    )
```

```python
import functools

import jax
import jax.numpy as jnp
from jax import lax
from jax.experimental import pallas as pl
from jax.experimental.pallas import tpu as pltpu
from jax.sharding import PartitionSpec as P

HEAD = 64
CHUNK = 64
TOKEN_PARTS = 2
PAIR = 128

NORM_EPS = 1e-06
GROUP_EPS = 1e-05
HEAD_EPS = 0.00064
KEY_EPS = 1e-06
MESH = pl.DeviceIdType.MESH
WIRE = jnp.bfloat16
VMEM_LIMIT = 60 * 1024 * 1024
F32 = jnp.float32
BF16 = jnp.bfloat16

NN = (((1,), (0,)), ((), ()))
NT = (((1,), (1,)), ((), ()))
TN = (((0,), (0,)), ((), ()))


def parts(x, count):
    out = []
    for _ in range(count - 1):
        piece = x.astype(BF16)
        out.append(piece)
        x = x - piece.astype(F32)
    out.append(x.astype(BF16))
    return out


def dot(a, b, dims=NN):
    return lax.dot_general(a, b, dims, preferred_element_type=F32)


def mm_left(a, b, dims=NN, count=2):
    pieces = [dot(piece, b, dims) for piece in parts(a, count)]
    return functools.reduce(jnp.add, pieces)


def split(x):
    high = x.astype(BF16)
    return high, (x - high.astype(F32)).astype(BF16)


def concat(pieces, axis=0):
    return jnp.concatenate(pieces, axis=axis)


def iota2(rows, cols):
    return (
        lax.broadcasted_iota(jnp.int32, (rows, cols), 0),
        lax.broadcasted_iota(jnp.int32, (rows, cols), 1),
    )


def head_blocks(width):
    row, col = iota2(width, width)
    return (row // HEAD) == (col // HEAD)


def own_head(shape):
    row, col = iota2(*shape)
    return (row // HEAD) == ((col % PAIR) // HEAD)


def diagonal(x):
    lane = lax.broadcasted_iota(jnp.int32, x.shape, 1)
    zero = jnp.zeros_like(x)
    return concat([jnp.where(lane < HEAD, x, zero), jnp.where(lane < HEAD, zero, x)])


def spread_pair(x):
    return concat([diagonal(x[:, :PAIR]), diagonal(x[:, PAIR:])], axis=1)


def compose(later, earlier):
    high, low = split(later[:, PAIR:])
    early_high, early_low = split(earlier)
    both = dot(concat([high, low]), spread_pair(early_high))
    out = both[:HEAD] + both[HEAD:] + dot(high, spread_pair(early_low))
    return concat([out[:, :PAIR] + later[:, :PAIR], out[:, PAIR:]], axis=1)


def layer_kernel(
    n_sp, n_tp,
    gain_hbm, kgain_hbm, bias_hbm, taps_hbm, ggain_hbm, gshift_hbm, hgain_hbm,
    tok_hbm, shift_hbm, extra_hbm, wcv, wcg, wk, wr, wd, we, wv, wg, wco, wao,
    out,
    gain, kgain, bias, taps, ggain, gshift, hgain,
    tok, shift, extra, cv_buf, cg_buf, k_buf, r_buf, d_buf, e_buf, v_buf, g_buf, co_buf, ao_buf,
    conv_in, extended, halo, own_map, partner_map, pair_map, early_map, maps, windows, state, reach, entered,
    local_read, carried, conv_out, mix_out, conv_slots, mix_slots,
    weight_sem, halo_sem, pair_sem, map_send, map_recv, cross_send, conv_send, conv_recv, mix_send, mix_recv,
):
    sp, tp = lax.axis_index("sp"), lax.axis_index("tp")
    part = tok_hbm.shape[0] // TOKEN_PARTS
    order = dict(gain=(gain_hbm, gain))
    for index in range(TOKEN_PARTS):
        span = pl.ds(index * part, part)
        order["tok" + str(index)] = (tok_hbm.at[span], tok.at[span])
    order.update(
        k=(wk, k_buf), kgain=(kgain_hbm, kgain), d=(wd, d_buf), bias=(bias_hbm, bias),
        shift=(shift_hbm, shift), extra=(extra_hbm, extra), e=(we, e_buf), v=(wv, v_buf),
        cv=(wcv, cv_buf), cg=(wcg, cg_buf), r=(wr, r_buf), g=(wg, g_buf),
        taps=(taps_hbm, taps), ggain=(ggain_hbm, ggain), gshift=(gshift_hbm, gshift),
        hgain=(hgain_hbm, hgain), co=(wco, co_buf), ao=(wao, ao_buf),
    )
    copies = {}
    for index, (key, (source, buffer)) in enumerate(order.items()):
        copies[key] = pltpu.make_async_copy(source, buffer, weight_sem.at[index])

    def begin(*keys):
        for key in keys:
            copies[key].start()

    def arrive(*keys):
        for key in keys:
            copies[key].wait()

    token_keys = ["tok" + str(index) for index in range(TOKEN_PARTS)]
    begin("gain", *token_keys, "k", "kgain", "d", "bias", "shift", "extra", "e", "v")
    barrier = pltpu.get_barrier_semaphore()
    for step in range(1, n_sp):
        pl.semaphore_signal(
            barrier, inc=1, device_id=(lax.rem(sp + step, n_sp), tp), device_id_type=MESH
        )
    for step in range(1, n_tp):
        pl.semaphore_signal(
            barrier, inc=1, device_id=(sp, lax.rem(tp + step, n_tp)), device_id_type=MESH
        )
    rows = tok.shape[0]
    channels = conv_in.shape[1]
    width = local_read.shape[1]
    heads = width // HEAD
    pairs = rows // PAIR
    halo_rows = halo.shape[0]
    groups = n_sp // 2
    group, parity = sp // 2, lax.rem(sp, 2)
    first_member = parity == 0
    quarters = []
    arrive("gain")
    for index, key in enumerate(token_keys):
        arrive(key)
        x = tok[index * part:(index + 1) * part].astype(F32)
        quarters.append(
            (
                x * lax.rsqrt(jnp.mean(x * x, axis=-1, keepdims=True) + NORM_EPS) * gain[...]
            ).astype(BF16)
        )
    begin("cv", "cg", "r", "g", "taps", "ggain", "gshift", "hgain")
    middle_part = TOKEN_PARTS // 2
    halves = [concat(quarters[:middle_part]), concat(quarters[middle_part:])]
    normed = concat(halves)

    def kept(x):
        return x.astype(BF16).astype(F32)

    def project(weight):
        return concat([dot(half, weight[...]) for half in halves])

    arrive("k", "d")
    key_all, slope = kept(dot(normed, k_buf[...])), kept(dot(normed, d_buf[...]))
    arrive("bias", "shift", "extra", "kgain", "e", "v")
    begin("co", "ao")
    rate = kept(project(e_buf))
    same_head = head_blocks(width)
    ones = jnp.where(same_head, 1.0, 0.0).astype(BF16)
    row, col = iota2(width, width)
    centre = (jnp.where(row == col, 1.0, 0.0) - jnp.where(same_head, 1.0 / HEAD, 0.0)).astype(BF16)
    logits = slope + bias[...] + shift[...]
    decay = jax.nn.sigmoid(logits) * (-0.6065306597126334) + extra[...]
    row, col = iota2(PAIR, 2 * PAIR)
    col = col % PAIR
    tri = jnp.where(((row // CHUNK) == (col // CHUNK)) & (row >= col), 1.0, 0.0).astype(BF16)
    cum = concat(
        [dot(tri, concat(split(decay[p:p + PAIR]))) for p in range(0, rows, PAIR)]
    )
    unit = key_all * kgain[...]
    unit = unit * lax.rsqrt(dot((unit * unit).astype(BF16), ones) + KEY_EPS)
    value = project(v_buf).astype(BF16)
    erase = -(unit * jax.nn.sigmoid(rate))
    value_high, value_low = split(dot(value, centre))
    chunks = rows // CHUNK
    groups_of = width // PAIR

    def by_chunk(row_of):
        return concat(
            [jnp.broadcast_to(row_of(c), (CHUNK, width)) for c in range(0, rows, CHUNK)]
        )

    def middle(c):
        return cum[c + CHUNK // 2 - 1:c + CHUNK // 2]

    def last(c):
        return cum[c + CHUNK - 1:c + CHUNK]

    mid = by_chunk(middle)
    from_start = by_chunk(lambda c: jnp.exp(middle(c)))
    to_end = by_chunk(lambda c: jnp.exp(last(c) - middle(c)))
    up = jnp.exp(mid - cum)
    left_unit = unit * jnp.exp(cum - decay - mid)
    query_unit = (left_unit * from_start).astype(BF16)
    left_unit = left_unit.astype(BF16)
    right_erase, right_key = erase * up, key_all * up
    kept_erase, kept_key = (right_erase * to_end).astype(BF16), (right_key * to_end).astype(BF16)
    right_erase, right_key = right_erase.astype(BF16), right_key.astype(BF16)
    units = [(c, g) for c in range(chunks) for g in range(groups_of)]

    def piece(values, unit_index):
        c, g = unit_index
        return values[c * CHUNK:(c + 1) * CHUNK, g * PAIR:(g + 1) * PAIR]

    row, col = iota2(CHUNK, PAIR)
    col = col % CHUNK
    strict, inclusive = row > col, row >= col
    eye = jnp.where(row == col, 1.0, 0.0)
    rights = [
        concat([diagonal(piece(right_erase, u)), diagonal(piece(right_key, u))]) for u in units
    ]
    products = [dot(piece(left_unit, u), right, NT) for u, right in zip(units, rights)]
    lower = [jnp.where(strict, product[:, :PAIR], 0.0) for product in products]
    mixes = [jnp.where(strict, product[:, PAIR:], 0.0).astype(BF16) for product in products]
    value_diagonals = [
        concat([diagonal(piece(value_high, u)), diagonal(piece(value_low, u))]) for u in units
    ]
    mixed = [
        dot(concat([mix, mix], axis=1), both) for mix, both in zip(mixes, value_diagonals)
    ]
    def within(size):
        return (row // size) == (col // size)

    def powers(left, right):
        return dot(left, concat([diagonal(right), diagonal(left)], axis=1))

    step = [jnp.where(within(4), low, 0.0) for low in lower]
    inverse = [eye + s for s in step]
    narrow = [s.astype(BF16) for s in step]
    square = [dot(s, diagonal(s)).astype(BF16) for s in narrow]
    inverse = [
        inv + dot(s, diagonal(inv.astype(BF16))) for inv, s in zip(inverse, square)
    ]
    narrow = [inv.astype(BF16) for inv in inverse]
    step = [
        dot(inv, diagonal(jnp.where(within(16) & ~within(4), low, 0.0).astype(BF16))).astype(BF16)
        for inv, low in zip(narrow, lower)
    ]
    both = [powers(s, inv) for s, inv in zip(step, narrow)]
    inverse = [inv + pair[:, :PAIR] for inv, pair in zip(inverse, both)]
    square = [pair[:, PAIR:].astype(BF16) for pair in both]
    inverse = [
        (inv + dot(s, diagonal(inv.astype(BF16)))).astype(BF16) for inv, s in zip(inverse, square)
    ]
    sides = [
        spread_pair(concat([mix.astype(BF16), piece(query_unit, u)], axis=1))
        for mix, u in zip(mixed, units)
    ]
    outer = [diagonal(jnp.where(within(16), 0.0, low).astype(BF16)) for low in lower]
    step = [dot(inv, far).astype(BF16) for inv, far in zip(inverse, outer)]
    solved = [dot(inv, side) for inv, side in zip(inverse, sides)]
    square = [dot(s, diagonal(s)).astype(BF16) for s in step]
    solved = [
        part + dot(s, spread_pair(part.astype(BF16))) for s, part in zip(step, solved)
    ]
    solved = [
        (part + dot(s, spread_pair(part.astype(BF16)))).astype(BF16)
        for s, part in zip(square, solved)
    ]
    nothing = jnp.zeros((CHUNK, PAIR), BF16)
    lane = lax.broadcasted_iota(jnp.int32, (HEAD, 2 * PAIR), 1)
    first_head = (lane % PAIR) < HEAD
    blocks = {}
    for index, u in enumerate(units):
        c, g = u
        left = concat([piece(kept_erase, u), piece(kept_key, u), piece(kept_key, u)])
        right = concat(
            [
                solved[index],
                concat([piece(value_high, u), nothing], axis=1),
                concat([piece(value_low, u), nothing], axis=1),
            ]
        )
        product = dot(left, right, TN)
        product = jnp.where(first_head, product[:HEAD], product[HEAD:])
        stay = jnp.exp(last(c * CHUNK)[:, g * PAIR:(g + 1) * PAIR])
        blocks[u] = concat([product[:, :PAIR], product[:, PAIR:] + eye * stay], axis=1)
    spans = {}
    for c in range(chunks):
        for g in range(groups_of):
            spans[c, c + 1, g] = blocks[c, g]
    size = 1
    while size < chunks:
        for c in range(0, chunks, 2 * size):
            for g in range(groups_of):
                spans[c, c + 2 * size, g] = compose(
                    spans[c + size, c + 2 * size, g], spans[c, c + size, g]
                )
        size *= 2
    totals = [spans[0, chunks, g] for g in range(groups_of)]
    own_total = concat(
        [
            concat([totals[g][:, :PAIR] for g in range(groups_of)], axis=1),
            concat([totals[g][:, PAIR:] for g in range(groups_of)], axis=1),
        ]
    ).astype(WIRE)
    own_map[...] = own_total

    pl.semaphore_wait(barrier, n_sp + n_tp - 2)
    origin = group == 0
    leads = origin & first_member

    def pair_part(side):
        span_of = pl.ds(side * HEAD, HEAD)
        return pltpu.make_async_remote_copy(
            src_ref=own_map.at[span_of], dst_ref=partner_map.at[span_of],
            send_sem=pair_sem.at[side], recv_sem=pair_sem.at[2 + side],
            device_id=(sp + 1 - 2 * parity, tp), device_id_type=MESH,
        )

    @pl.when((group > 0) | first_member)
    def _():
        pair_part(0).start()

    @pl.when(group > 0)
    def _():
        pair_part(1).start()

    arrive("cv", "cg")
    both = concat([cv_buf[...], cg_buf[...]], axis=1)
    conv_pair = kept(concat([dot(part, both) for part in halves]))
    conv_rows = (
        conv_pair[:, :channels] * jax.nn.sigmoid(conv_pair[:, channels:])
    ).astype(BF16)
    conv_in[...] = conv_rows
    halo_copy = pltpu.make_async_remote_copy(
        src_ref=conv_in.at[pl.ds(rows - halo_rows, halo_rows)], dst_ref=halo,
        send_sem=halo_sem.at[0], recv_sem=halo_sem.at[1],
        device_id=(sp + 1, tp), device_id_type=MESH,
    )
    has_next = sp + 1 < n_sp

    @pl.when(has_next)
    def _():
        halo_copy.start()

    extended[halo_rows:, :] = conv_rows.astype(F32)

    arrive("r")
    receptance = kept(project(r_buf))
    left_read = receptance * jnp.exp(cum - mid)
    query_read = left_read * from_start
    left_read = left_read.astype(BF16)
    zeros = jnp.zeros((PAIR, PAIR), BF16)
    products = [dot(piece(left_read, u), right, NT) for u, right in zip(units, rights)]
    reads = []
    for product, end, both, u in zip(products, solved, value_diagonals, units):
        keys = jnp.where(inclusive, product[:, PAIR:], 0.0).astype(BF16)
        mix = concat(
            [jnp.where(inclusive, product[:, :PAIR], 0.0).astype(BF16), keys, keys], axis=1
        )
        stacked = concat(
            [spread_pair(end), concat([both, concat([zeros, zeros])], axis=1)]
        )
        reads.append(dot(mix, stacked))
    priors = {}
    for c in range(1, chunks):
        start, size = 0, chunks // 2
        while start < c:
            while start + size > c:
                size //= 2
            for g in range(groups_of):
                block = spans[start, start + size, g]
                priors[c, g] = block if start == 0 else compose(block, priors[c, g])
            start += size
    for index, u in enumerate(units):
        c, g = u
        near, far = reads[index][:, :PAIR], reads[index][:, PAIR:] + piece(query_read, u)
        if c > 0:
            moved = dot(far.astype(BF16), spread_pair(priors[u].astype(BF16)))
            near, far = near + moved[:, :PAIR], moved[:, PAIR:]
        span = slice(c * CHUNK, (c + 1) * CHUNK)
        lanes = slice(g * PAIR, (g + 1) * PAIR)
        local_read[span, lanes] = near
        carried[span, lanes] = far.astype(BF16)

    def by_pair(x):
        return [x[:, g * PAIR:(g + 1) * PAIR] for g in range(groups_of)]

    def chain(held, move):
        out = []
        for state_part, move_part in zip(by_pair(held), by_pair(move)):
            right = concat([diagonal(piece_of) for piece_of in split(state_part)])
            out.append(dot(concat([move_part, move_part], axis=1), right))
        return concat(out, axis=1)

    early_map[...] = own_map[...]

    @pl.when(parity == 1)
    def _():
        pair_part(0).wait_recv()
        early_map[:HEAD] = partner_map[:HEAD]

    def join(lead, follow, side):
        moved = chain(lead[side * HEAD:(side + 1) * HEAD].astype(F32), follow[HEAD:])
        if side == 0:
            moved = moved + follow[:HEAD].astype(F32)
        pair_map[side * HEAD:(side + 1) * HEAD] = moved.astype(WIRE)

    @pl.when(origin & (parity == 1))
    def _():
        join(early_map, own_map, 0)

    @pl.when(group > 0)
    def _():
        pair_part(1).wait_recv()

    @pl.when((group > 0) & (parity == 1))
    def _():
        early_map[HEAD:] = partner_map[HEAD:]
        join(early_map, own_map, 0)
        join(early_map, own_map, 1)

    @pl.when((group > 0) & first_member)
    def _():
        pair_part(0).wait_recv()
        join(own_map, partner_map, 0)
        join(own_map, partner_map, 1)

    hops = []
    while 2 ** len(hops) < groups:
        hops.append(2 ** len(hops))

    def hop(source, k, side, member=parity):
        span_of = pl.ds(side * HEAD, HEAD)
        return pltpu.make_async_remote_copy(
            src_ref=source.at[span_of], dst_ref=maps.at[k, span_of],
            send_sem=map_send.at[2 * k + side], recv_sem=map_recv.at[2 * k + side],
            device_id=(2 * (group + hops[k]) + member, tp), device_id_type=MESH,
        )

    def hop_across(k):
        return pltpu.make_async_remote_copy(
            src_ref=pair_map.at[pl.ds(0, HEAD)], dst_ref=maps.at[k, pl.ds(0, HEAD)],
            send_sem=cross_send.at[k], recv_sem=map_recv.at[2 * k],
            device_id=(2 * hops[k], tp), device_id_type=MESH,
        )

    sends = []
    for k, ahead in enumerate(hops):
        reached = group + ahead < groups
        sends.append((0, origin & (parity == 1), hop_across(k)))
        sends.append((0, origin & (parity == 1), hop(pair_map, k, 0)))
        source = pair_map if k == 0 else windows.at[k]
        sends.append((k, reached & (group >= 1), hop(source, k, 0)))
        if 2 * ahead < groups:
            sends.append((k, reached & (group >= ahead), hop(source, k, 1)))

    def send_step(step):
        for when, allowed, copy in sends:
            if when == step:
                pl.when(allowed)(copy.start)

    if hops:
        send_step(0)

    @pl.when(sp > 0)
    def _():
        halo_copy.wait_recv()
        extended[:halo_rows, :] = halo[...].astype(F32)

    @pl.when(sp == 0)
    def _():
        extended[:halo_rows, :] = jnp.zeros((halo_rows, channels), F32)


    def fold(block):
        for g in range(groups_of):
            lanes = slice(g * PAIR, (g + 1) * PAIR)
            right = spread_pair(concat([block[:HEAD, lanes], block[HEAD:, lanes]], axis=1))
            moved = dot(carried[:, lanes], right)
            local_read[:, lanes] = local_read[:, lanes] + moved[:, :PAIR]
            carried[:, lanes] = moved[:, PAIR:].astype(BF16)

    @pl.when(parity == 1)
    def _():
        fold(early_map)

    arrive("g", "hgain")
    gate = jax.nn.sigmoid(kept(project(g_buf))) * hgain[...]
    arrive("taps", "ggain", "gshift")
    tap_count = taps.shape[0]
    total = jnp.zeros((rows, channels), F32)
    for offset in range(tap_count):
        begin = halo_rows - tap_count + 1 + offset
        total = total + taps[offset:offset + 1, :] * extended[begin:begin + rows, :]
    means = jnp.where(head_blocks(channels), 1.0 / HEAD, 0.0).astype(BF16)
    centred = total - mm_left(total, means)
    scaled = centred * lax.rsqrt(mm_left(centred * centred, means) + GROUP_EPS)
    conv_out[...] = jax.nn.silu(scaled * ggain[...] + gshift[...]).astype(BF16)

    span = rows // n_tp

    def peer(step):
        if n_tp & (n_tp - 1):
            return lax.rem(tp + step, n_tp), lax.rem(tp - step + n_tp, n_tp)
        other, bit = tp, 1
        while bit < n_tp:
            if step & bit:
                other = other + bit - 2 * bit * lax.rem(tp // bit, 2)
            bit *= 2
        return other, other

    def spread(source, slots, send, recv):
        started = []
        for step in range(1, n_tp):
            target = peer(step)[0]
            begin = pl.multiple_of(target * span, span)
            copy = pltpu.make_async_remote_copy(
                src_ref=source.at[pl.ds(begin, span)], dst_ref=slots.at[step],
                send_sem=send.at[step], recv_sem=recv.at[step],
                device_id=(sp, target), device_id_type=MESH,
            )
            copy.start()
            started.append(copy)
        return started

    conv_copies = spread(conv_out, conv_slots, conv_send, conv_recv)

    own = pl.multiple_of(tp * span, span)

    def gather(result, source, slots, arriving, weight, depth, offset, count):
        def rows_of(owner):
            return pl.ds(pl.multiple_of(owner * depth + offset, PAIR), count)

        result = result + dot(source[pl.ds(own, span)], weight[rows_of(tp)])
        for step in range(1, n_tp):
            arriving[step - 1].wait_recv()
            result = result + dot(slots[step], weight[rows_of(peer(step)[1])])
        return result

    entered[...] = jnp.zeros_like(entered)
    for k, ahead in enumerate(hops):
        final = group < 2 * ahead
        following = 2 * ahead

        @pl.when(group >= ahead)
        def _():
            hop(pair_map, k, 0).wait_recv()

        @pl.when((group >= ahead) & final)
        def _():
            entered[...] = maps[k, :HEAD]

        if following < groups:
            @pl.when(group >= ahead)
            def _():
                arrived = maps[k, :HEAD].astype(F32)
                state[...] = arrived if k == 0 else chain(arrived, reach[...]) + state[...]

            @pl.when((group == 0) & (k == 0))
            def _():
                state[...] = jnp.zeros_like(state)

            @pl.when((group >= 1) & (group + following < groups))
            def _():
                windows[k + 1, :HEAD] = (
                    chain(state[...], pair_map[HEAD:]) + pair_map[:HEAD].astype(F32)
                ).astype(WIRE)

            if 2 * following < groups:
                @pl.when(group >= following)
                def _():
                    hop(pair_map, k, 1).wait_recv()
                    further = maps[k, HEAD:]
                    if k > 0:
                        further = chain(further.astype(F32), reach[...]).astype(WIRE)
                    reach[...] = further

                @pl.when((group >= following) & (group + following < groups))
                def _():
                    windows[k + 1, HEAD:] = chain(
                        reach[...].astype(F32), pair_map[HEAD:]
                    ).astype(WIRE)
            else:
                @pl.when(group >= following)
                def _():
                    hop(pair_map, k, 1).wait_recv()

            send_step(k + 1)

            @pl.when(group >= following)
            def _():
                fold(maps.at[k])

    head_means = jnp.where(head_blocks(PAIR), 1.0 / HEAD, 0.0).astype(BF16)
    mix_copies = []
    lanes_of = [slice(g * PAIR, (g + 1) * PAIR) for g in range(groups_of)]
    centred = [
        local_read[:, lanes] + dot(carried[:, lanes], diagonal(part))
        for lanes, part in zip(lanes_of, by_pair(entered[...]))
    ]
    power = [dot((read * read).astype(BF16), head_means) for read in centred]
    for g, lanes in enumerate(lanes_of):
        scaled = centred[g] * lax.rsqrt(power[g] + HEAD_EPS)
        mix_out[g] = (scaled * gate[:, lanes]).astype(BF16)
        mix_copies.append(
            spread(mix_out.at[g], mix_slots.at[g], mix_send.at[g], mix_recv.at[g])
        )
    arrive("co")
    result = gather(
        jnp.zeros(out.shape, F32), conv_out, conv_slots, conv_copies, co_buf, channels, 0, channels
    )

    arrive("ao")
    for g in range(groups_of):
        result = gather(
            result, mix_out.at[g], mix_slots.at[g], mix_copies[g], ao_buf, width, g * PAIR, PAIR
        )
    out[...] = result.astype(BF16)
    for copy in sum(mix_copies, conv_copies):
        copy.wait_send()

    @pl.when(has_next)
    def _():
        halo_copy.wait_send()

    for _, allowed, copy in sends:
        pl.when(allowed)(copy.wait_send)

    @pl.when((group > 0) | first_member)
    def _():
        pair_part(0).wait_send()

    @pl.when(group > 0)
    def _():
        pair_part(1).wait_send()


def local(
    n_sp, n_tp,
    tokens, input_norm_gain, convolution_value_weight, convolution_gate_weight,
    depthwise_taps_weight, convolution_group_gain, convolution_group_shift,
    receptance_weight, key_weight, value_weight, decay_weight, correction_rate_weight,
    output_gate_weight, key_prenorm_gain, decay_offset_bias, position_decay_shift,
    extra_log_decay, head_norm_gain, convolution_output_weight, attention_output_weight,
):
    rows, model = tokens.shape
    channels = convolution_value_weight.shape[1]
    width = key_weight.shape[1]
    vmem = pl.BlockSpec(memory_space=pltpu.VMEM)
    anywhere = pl.BlockSpec(memory_space=pl.ANY)

    def line(values):
        return values.reshape(1, -1)

    smalls = (
        line(input_norm_gain), line(key_prenorm_gain), line(decay_offset_bias),
        depthwise_taps_weight, line(convolution_group_gain), line(convolution_group_shift),
        line(head_norm_gain),
    )
    weights = (
        convolution_value_weight, convolution_gate_weight, key_weight, receptance_weight,
        decay_weight, correction_rate_weight, value_weight, output_gate_weight,
        convolution_output_weight, attention_output_weight,
    )
    span = rows // n_tp
    halo_rows = -(-(depthwise_taps_weight.shape[0] - 1) // 16) * 16
    hop_count = max(1, (n_sp // 2 - 1).bit_length())
    dma = pltpu.SemaphoreType.DMA
    map_shape = (2 * HEAD, width)
    return pl.pallas_call(
        functools.partial(layer_kernel, n_sp, n_tp),
        name="layer",
        out_shape=pltpu.VMEM((span, model), BF16),
        in_specs=[anywhere] * 20,
        out_specs=vmem,
        scratch_shapes=[pltpu.VMEM(small.shape, F32) for small in smalls]
        + [
            pltpu.VMEM(tokens.shape, BF16),
            pltpu.VMEM(position_decay_shift.shape, F32),
            pltpu.VMEM(extra_log_decay.shape, F32),
        ]
        + [pltpu.VMEM(weight.shape, BF16) for weight in weights]
        + [
            pltpu.VMEM((rows, channels), BF16),
            pltpu.VMEM((halo_rows + rows, channels), F32),
            pltpu.VMEM((halo_rows, channels), BF16),
            pltpu.VMEM(map_shape, WIRE),
            pltpu.VMEM(map_shape, WIRE),
            pltpu.VMEM(map_shape, WIRE),
            pltpu.VMEM(map_shape, WIRE),
            pltpu.VMEM((hop_count,) + map_shape, WIRE),
            pltpu.VMEM((hop_count,) + map_shape, WIRE),
            pltpu.VMEM((HEAD, width), F32),
            pltpu.VMEM((HEAD, width), WIRE),
            pltpu.VMEM((HEAD, width), WIRE),
            pltpu.VMEM((rows, width), F32),
            pltpu.VMEM((rows, width), BF16),
            pltpu.VMEM((rows, channels), BF16),
            pltpu.VMEM((width // PAIR, rows, PAIR), BF16),
            pltpu.VMEM((n_tp, span, channels), BF16),
            pltpu.VMEM((width // PAIR, n_tp, span, PAIR), BF16),
            dma((24,)), dma((2,)), dma((4,)), dma((2 * hop_count,)), dma((2 * hop_count,)),
            dma((hop_count,)),
            dma((n_tp,)), dma((n_tp,)),
            dma((width // PAIR, n_tp)), dma((width // PAIR, n_tp)),
        ],
        compiler_params=pltpu.CompilerParams(
            collective_id=0, has_side_effects=True, vmem_limit_bytes=VMEM_LIMIT
        ),
    )(
        *smalls, tokens, position_decay_shift, extra_log_decay, *weights,
    )


def solution(mesh):
    in_specs = (
        P("sp", None),
        P(),
        P(None, "tp"),
        P(None, "tp"),
        P(None, "tp"),
        P("tp"),
        P("tp"),
        P(None, "tp"),
        P(None, "tp"),
        P(None, "tp"),
        P(None, "tp"),
        P(None, "tp"),
        P(None, "tp"),
        P("tp"),
        P("tp"),
        P("sp", "tp"),
        P("sp", "tp"),
        P("tp"),
        P(),
        P(),
    )
    body = functools.partial(local, mesh.shape["sp"], mesh.shape["tp"])
    return jax.shard_map(
        body, mesh=mesh, in_specs=in_specs, out_specs=P(("sp", "tp"), None), check_vma=False
    )
```

```python
import functools

import jax
import jax.numpy as jnp
from jax import lax
from jax.experimental import pallas as pl
from jax.experimental.pallas import tpu as pltpu
from jax.sharding import PartitionSpec as P

HEAD = 64
CHUNK = 64
TOKEN_PARTS = 2
PAIR = 128

NORM_EPS = 1e-06
GROUP_EPS = 1e-05
HEAD_EPS = 0.00064
KEY_EPS = 1e-06
MESH = pl.DeviceIdType.MESH
WIRE = jnp.bfloat16
VMEM_LIMIT = 60 * 1024 * 1024
F32 = jnp.float32
BF16 = jnp.bfloat16

NN = (((1,), (0,)), ((), ()))
NT = (((1,), (1,)), ((), ()))
TN = (((0,), (0,)), ((), ()))


def parts(x, count):
    out = []
    for _ in range(count - 1):
        piece = x.astype(BF16)
        out.append(piece)
        x = x - piece.astype(F32)
    out.append(x.astype(BF16))
    return out


def dot(a, b, dims=NN):
    return lax.dot_general(a, b, dims, preferred_element_type=F32)


def mm_left(a, b, dims=NN, count=2):
    pieces = [dot(piece, b, dims) for piece in parts(a, count)]
    return functools.reduce(jnp.add, pieces)


def split(x):
    high = x.astype(BF16)
    return high, (x - high.astype(F32)).astype(BF16)


def concat(pieces, axis=0):
    return jnp.concatenate(pieces, axis=axis)


def iota2(rows, cols):
    return (
        lax.broadcasted_iota(jnp.int32, (rows, cols), 0),
        lax.broadcasted_iota(jnp.int32, (rows, cols), 1),
    )


def head_blocks(width):
    row, col = iota2(width, width)
    return (row // HEAD) == (col // HEAD)


def own_head(shape):
    row, col = iota2(*shape)
    return (row // HEAD) == ((col % PAIR) // HEAD)


def diagonal(x):
    lane = lax.broadcasted_iota(jnp.int32, x.shape, 1)
    zero = jnp.zeros_like(x)
    return concat([jnp.where(lane < HEAD, x, zero), jnp.where(lane < HEAD, zero, x)])


def spread_pair(x):
    return concat([diagonal(x[:, :PAIR]), diagonal(x[:, PAIR:])], axis=1)


def compose(later, earlier):
    high, low = split(later[:, PAIR:])
    early_high, early_low = split(earlier)
    both = dot(concat([high, low]), spread_pair(early_high))
    out = both[:HEAD] + both[HEAD:] + dot(high, spread_pair(early_low))
    return concat([out[:, :PAIR] + later[:, :PAIR], out[:, PAIR:]], axis=1)


def layer_kernel(
    n_sp, n_tp,
    gain_hbm, kgain_hbm, bias_hbm, taps_hbm, ggain_hbm, gshift_hbm, hgain_hbm,
    tok_hbm, shift_hbm, extra_hbm, wcv, wcg, wk, wr, wd, we, wv, wg, wco, wao,
    out,
    gain, kgain, bias, taps, ggain, gshift, hgain,
    tok, shift, extra, cv_buf, cg_buf, k_buf, r_buf, d_buf, e_buf, v_buf, g_buf, co_buf, ao_buf,
    conv_in, extended, halo, own_map, partner_map, pair_map, early_map, maps, windows, state, reach, entered,
    local_read, carried, conv_out, mix_out, conv_slots, mix_slots,
    weight_sem, halo_sem, pair_sem, map_send, map_recv, cross_send, conv_send, conv_recv, mix_send, mix_recv,
):
    sp, tp = lax.axis_index("sp"), lax.axis_index("tp")
    part = tok_hbm.shape[0] // TOKEN_PARTS
    order = dict(gain=(gain_hbm, gain))
    for index in range(TOKEN_PARTS):
        span = pl.ds(index * part, part)
        order["tok" + str(index)] = (tok_hbm.at[span], tok.at[span])
    order.update(
        k=(wk, k_buf), kgain=(kgain_hbm, kgain), d=(wd, d_buf), bias=(bias_hbm, bias),
        shift=(shift_hbm, shift), extra=(extra_hbm, extra), e=(we, e_buf), v=(wv, v_buf),
        cv=(wcv, cv_buf), cg=(wcg, cg_buf), r=(wr, r_buf), g=(wg, g_buf),
        taps=(taps_hbm, taps), ggain=(ggain_hbm, ggain), gshift=(gshift_hbm, gshift),
        hgain=(hgain_hbm, hgain), co=(wco, co_buf), ao=(wao, ao_buf),
    )
    together = (
        ("gain", "tok0"), ("tok1",), ("k", "d"), ("bias", "shift", "extra", "kgain", "e"), ("v",),
        ("cv", "cg"), ("r",), ("taps", "ggain", "gshift"), ("g", "hgain"), ("co",), ("ao",),
    )
    copies = {}
    for index, keys in enumerate(together):
        for key in keys:
            source, buffer = order[key]
            copies[key] = pltpu.make_async_copy(source, buffer, weight_sem.at[index])

    def begin(*keys):
        for key in keys:
            copies[key].start()

    def arrive(*keys):
        for key in keys:
            copies[key].wait()

    token_keys = ["tok" + str(index) for index in range(TOKEN_PARTS)]
    begin("gain", *token_keys, "k", "kgain", "d", "bias", "shift", "extra", "e", "v")
    barrier = pltpu.get_barrier_semaphore()
    for step in range(1, n_sp):
        pl.semaphore_signal(
            barrier, inc=1, device_id=(lax.rem(sp + step, n_sp), tp), device_id_type=MESH
        )
    for step in range(1, n_tp):
        pl.semaphore_signal(
            barrier, inc=1, device_id=(sp, lax.rem(tp + step, n_tp)), device_id_type=MESH
        )
    rows = tok.shape[0]
    channels = conv_in.shape[1]
    width = local_read.shape[1]
    heads = width // HEAD
    pairs = rows // PAIR
    halo_rows = halo.shape[0]
    groups = n_sp // 2
    group, parity = sp // 2, lax.rem(sp, 2)
    first_member = parity == 0
    quarters = []
    for index, key in enumerate(token_keys):
        arrive(*(("gain", key) if index == 0 else (key,)))
        x = tok[index * part:(index + 1) * part].astype(F32)
        quarters.append(
            (
                x * lax.rsqrt(jnp.mean(x * x, axis=-1, keepdims=True) + NORM_EPS) * gain[...]
            ).astype(BF16)
        )
    begin("cv", "cg", "r", "g", "taps", "ggain", "gshift", "hgain")
    middle_part = TOKEN_PARTS // 2
    halves = [concat(quarters[:middle_part]), concat(quarters[middle_part:])]
    normed = concat(halves)

    def kept(x):
        return x.astype(BF16).astype(F32)

    def project(weight):
        return concat([dot(half, weight[...]) for half in halves])

    arrive("k", "d")
    key_all, slope = kept(dot(normed, k_buf[...])), kept(dot(normed, d_buf[...]))
    arrive("bias", "shift", "extra", "kgain", "e")
    rate = kept(project(e_buf))
    same_head = head_blocks(width)
    ones = jnp.where(same_head, 1.0, 0.0).astype(BF16)
    row, col = iota2(width, width)
    centre = (jnp.where(row == col, 1.0, 0.0) - jnp.where(same_head, 1.0 / HEAD, 0.0)).astype(BF16)
    logits = slope + bias[...] + shift[...]
    decay = jax.nn.sigmoid(logits) * (-0.6065306597126334) + extra[...]
    row, col = iota2(PAIR, 2 * PAIR)
    col = col % PAIR
    tri = jnp.where(((row // CHUNK) == (col // CHUNK)) & (row >= col), 1.0, 0.0).astype(BF16)
    cum = concat(
        [dot(tri, concat(split(decay[p:p + PAIR]))) for p in range(0, rows, PAIR)]
    )
    unit = key_all * kgain[...]
    unit = unit * lax.rsqrt(dot((unit * unit).astype(BF16), ones) + KEY_EPS)
    erase = -(unit * jax.nn.sigmoid(rate))
    chunks = rows // CHUNK
    groups_of = width // PAIR

    def by_chunk(row_of):
        return concat(
            [jnp.broadcast_to(row_of(c), (CHUNK, width)) for c in range(0, rows, CHUNK)]
        )

    def middle(c):
        return cum[c + CHUNK // 2 - 1:c + CHUNK // 2]

    def last(c):
        return cum[c + CHUNK - 1:c + CHUNK]

    mid = by_chunk(middle)
    from_start = by_chunk(lambda c: jnp.exp(middle(c)))
    to_end = by_chunk(lambda c: jnp.exp(last(c) - middle(c)))
    up = jnp.exp(mid - cum)
    left_unit = unit * jnp.exp(cum - decay - mid)
    query_unit = (left_unit * from_start).astype(BF16)
    left_unit = left_unit.astype(BF16)
    right_erase, right_key = erase * up, key_all * up
    kept_erase, kept_key = (right_erase * to_end).astype(BF16), (right_key * to_end).astype(BF16)
    right_erase, right_key = right_erase.astype(BF16), right_key.astype(BF16)
    units = [(c, g) for c in range(chunks) for g in range(groups_of)]

    def piece(values, unit_index):
        c, g = unit_index
        return values[c * CHUNK:(c + 1) * CHUNK, g * PAIR:(g + 1) * PAIR]

    row, col = iota2(CHUNK, PAIR)
    col = col % CHUNK
    strict, inclusive = row > col, row >= col
    eye = jnp.where(row == col, 1.0, 0.0)
    rights = [
        concat([diagonal(piece(right_erase, u)), diagonal(piece(right_key, u))]) for u in units
    ]
    products = [dot(piece(left_unit, u), right, NT) for u, right in zip(units, rights)]
    lower = [jnp.where(strict, product[:, :PAIR], 0.0) for product in products]
    mixes = [jnp.where(strict, product[:, PAIR:], 0.0).astype(BF16) for product in products]
    arrive("v")
    begin("co", "ao")
    slices = [slice(b, b + 2 * PAIR) for b in range(0, normed.shape[1], 2 * PAIR)]
    value_sums = [None, None]

    def value_some(count):
        for span in [slices.pop(0) for _ in range(min(count, len(slices)))]:
            for index, half in enumerate(halves):
                part_of = dot(half[:, span], v_buf[span, :])
                held = value_sums[index]
                value_sums[index] = part_of if held is None else held + part_of

    def within(size):
        return (row // size) == (col // size)

    def powers(left, right):
        return dot(left, concat([diagonal(right), diagonal(left)], axis=1))

    step = [jnp.where(within(4), low, 0.0) for low in lower]
    inverse = [eye + s for s in step]
    narrow = [s.astype(BF16) for s in step]
    square = [dot(s, diagonal(s)).astype(BF16) for s in narrow]
    value_some(3)
    inverse = [
        inv + dot(s, diagonal(inv.astype(BF16))) for inv, s in zip(inverse, square)
    ]
    value_some(3)
    narrow = [inv.astype(BF16) for inv in inverse]
    step = [
        dot(inv, diagonal(jnp.where(within(16) & ~within(4), low, 0.0).astype(BF16))).astype(BF16)
        for inv, low in zip(narrow, lower)
    ]
    value_some(len(slices))
    both = [powers(s, inv) for s, inv in zip(step, narrow)]
    value_high, value_low = split(dot(concat(value_sums).astype(BF16), centre))
    inverse = [inv + pair[:, :PAIR] for inv, pair in zip(inverse, both)]
    square = [pair[:, PAIR:].astype(BF16) for pair in both]
    inverse = [
        (inv + dot(s, diagonal(inv.astype(BF16)))).astype(BF16) for inv, s in zip(inverse, square)
    ]
    value_diagonals = [
        concat([diagonal(piece(value_high, u)), diagonal(piece(value_low, u))]) for u in units
    ]
    mixed = [
        dot(concat([mix, mix], axis=1), held) for mix, held in zip(mixes, value_diagonals)
    ]
    outer = [diagonal(jnp.where(within(16), 0.0, low).astype(BF16)) for low in lower]
    step = [dot(inv, far).astype(BF16) for inv, far in zip(inverse, outer)]
    sides = [
        spread_pair(concat([mix.astype(BF16), piece(query_unit, u)], axis=1))
        for mix, u in zip(mixed, units)
    ]
    solved = [dot(inv, side) for inv, side in zip(inverse, sides)]
    square = [dot(s, diagonal(s)).astype(BF16) for s in step]
    solved = [
        part + dot(s, spread_pair(part.astype(BF16))) for s, part in zip(step, solved)
    ]
    solved = [
        (part + dot(s, spread_pair(part.astype(BF16)))).astype(BF16)
        for s, part in zip(square, solved)
    ]
    nothing = jnp.zeros((CHUNK, PAIR), BF16)
    lane = lax.broadcasted_iota(jnp.int32, (HEAD, 2 * PAIR), 1)
    first_head = (lane % PAIR) < HEAD
    blocks = {}
    for index, u in enumerate(units):
        c, g = u
        left = concat([piece(kept_erase, u), piece(kept_key, u), piece(kept_key, u)])
        right = concat(
            [
                solved[index],
                concat([piece(value_high, u), nothing], axis=1),
                concat([piece(value_low, u), nothing], axis=1),
            ]
        )
        product = dot(left, right, TN)
        product = jnp.where(first_head, product[:HEAD], product[HEAD:])
        stay = jnp.exp(last(c * CHUNK)[:, g * PAIR:(g + 1) * PAIR])
        blocks[u] = concat([product[:, :PAIR], product[:, PAIR:] + eye * stay], axis=1)
    spans = {}
    for c in range(chunks):
        for g in range(groups_of):
            spans[c, c + 1, g] = blocks[c, g]
    size = 1
    while size < chunks:
        for c in range(0, chunks, 2 * size):
            for g in range(groups_of):
                spans[c, c + 2 * size, g] = compose(
                    spans[c + size, c + 2 * size, g], spans[c, c + size, g]
                )
        size *= 2
    totals = [spans[0, chunks, g] for g in range(groups_of)]
    own_total = concat(
        [
            concat([totals[g][:, :PAIR] for g in range(groups_of)], axis=1),
            concat([totals[g][:, PAIR:] for g in range(groups_of)], axis=1),
        ]
    ).astype(WIRE)
    own_map[...] = own_total

    pl.semaphore_wait(barrier, n_sp + n_tp - 2)
    origin = group == 0
    leads = origin & first_member

    def pair_part(side):
        span_of = pl.ds(side * HEAD, HEAD)
        return pltpu.make_async_remote_copy(
            src_ref=own_map.at[span_of], dst_ref=partner_map.at[span_of],
            send_sem=pair_sem.at[side], recv_sem=pair_sem.at[2 + side],
            device_id=(sp + 1 - 2 * parity, tp), device_id_type=MESH,
        )

    @pl.when((group > 0) | first_member)
    def _():
        pair_part(0).start()

    @pl.when(group > 0)
    def _():
        pair_part(1).start()

    arrive("cv", "cg")
    both = concat([cv_buf[...], cg_buf[...]], axis=1)
    conv_pair = kept(concat([dot(part, both) for part in halves]))
    conv_rows = (
        conv_pair[:, :channels] * jax.nn.sigmoid(conv_pair[:, channels:])
    ).astype(BF16)
    conv_in[...] = conv_rows
    halo_copy = pltpu.make_async_remote_copy(
        src_ref=conv_in.at[pl.ds(rows - halo_rows, halo_rows)], dst_ref=halo,
        send_sem=halo_sem.at[0], recv_sem=halo_sem.at[1],
        device_id=(sp + 1, tp), device_id_type=MESH,
    )
    has_next = sp + 1 < n_sp

    @pl.when(has_next)
    def _():
        halo_copy.start()

    extended[halo_rows:, :] = conv_rows.astype(F32)

    arrive("r")
    receptance = kept(project(r_buf))
    left_read = receptance * jnp.exp(cum - mid)
    query_read = left_read * from_start
    left_read = left_read.astype(BF16)
    zeros = jnp.zeros((PAIR, PAIR), BF16)
    products = [dot(piece(left_read, u), right, NT) for u, right in zip(units, rights)]
    reads = []
    for product, end, both, u in zip(products, solved, value_diagonals, units):
        keys = jnp.where(inclusive, product[:, PAIR:], 0.0).astype(BF16)
        mix = concat(
            [jnp.where(inclusive, product[:, :PAIR], 0.0).astype(BF16), keys, keys], axis=1
        )
        stacked = concat(
            [spread_pair(end), concat([both, concat([zeros, zeros])], axis=1)]
        )
        reads.append(dot(mix, stacked))
    priors = {}
    for c in range(1, chunks):
        start, size = 0, chunks // 2
        while start < c:
            while start + size > c:
                size //= 2
            for g in range(groups_of):
                block = spans[start, start + size, g]
                priors[c, g] = block if start == 0 else compose(block, priors[c, g])
            start += size
    for index, u in enumerate(units):
        c, g = u
        near, far = reads[index][:, :PAIR], reads[index][:, PAIR:] + piece(query_read, u)
        if c > 0:
            moved = dot(far.astype(BF16), spread_pair(priors[u].astype(BF16)))
            near, far = near + moved[:, :PAIR], moved[:, PAIR:]
        span = slice(c * CHUNK, (c + 1) * CHUNK)
        lanes = slice(g * PAIR, (g + 1) * PAIR)
        local_read[span, lanes] = near
        carried[span, lanes] = far.astype(BF16)

    def by_pair(x):
        return [x[:, g * PAIR:(g + 1) * PAIR] for g in range(groups_of)]

    def chain(held, move):
        out = []
        for state_part, move_part in zip(by_pair(held), by_pair(move)):
            right = concat([diagonal(piece_of) for piece_of in split(state_part)])
            out.append(dot(concat([move_part, move_part], axis=1), right))
        return concat(out, axis=1)

    early_map[...] = own_map[...]

    @pl.when(parity == 1)
    def _():
        pair_part(0).wait_recv()
        early_map[:HEAD] = partner_map[:HEAD]

    def join(lead, follow, side):
        moved = chain(lead[side * HEAD:(side + 1) * HEAD].astype(F32), follow[HEAD:])
        if side == 0:
            moved = moved + follow[:HEAD].astype(F32)
        pair_map[side * HEAD:(side + 1) * HEAD] = moved.astype(WIRE)

    @pl.when(origin & (parity == 1))
    def _():
        join(early_map, own_map, 0)

    @pl.when(group > 0)
    def _():
        pair_part(1).wait_recv()

    @pl.when((group > 0) & (parity == 1))
    def _():
        early_map[HEAD:] = partner_map[HEAD:]
        join(early_map, own_map, 0)
        join(early_map, own_map, 1)

    @pl.when((group > 0) & first_member)
    def _():
        pair_part(0).wait_recv()
        join(own_map, partner_map, 0)
        join(own_map, partner_map, 1)

    hops = []
    while 2 ** len(hops) < groups:
        hops.append(2 ** len(hops))

    def hop(source, k, side, member=parity):
        span_of = pl.ds(side * HEAD, HEAD)
        return pltpu.make_async_remote_copy(
            src_ref=source.at[span_of], dst_ref=maps.at[k, span_of],
            send_sem=map_send.at[2 * k + side], recv_sem=map_recv.at[2 * k + side],
            device_id=(2 * (group + hops[k]) + member, tp), device_id_type=MESH,
        )

    def hop_across(k):
        return pltpu.make_async_remote_copy(
            src_ref=pair_map.at[pl.ds(0, HEAD)], dst_ref=maps.at[k, pl.ds(0, HEAD)],
            send_sem=cross_send.at[k], recv_sem=map_recv.at[2 * k],
            device_id=(2 * hops[k], tp), device_id_type=MESH,
        )

    sends = []
    for k, ahead in enumerate(hops):
        reached = group + ahead < groups
        sends.append((0, origin & (parity == 1), hop_across(k)))
        sends.append((0, origin & (parity == 1), hop(pair_map, k, 0)))
        source = pair_map if k == 0 else windows.at[k]
        sends.append((k, reached & (group >= 1), hop(source, k, 0)))
        if 2 * ahead < groups:
            sends.append((k, reached & (group >= ahead), hop(source, k, 1)))

    def send_step(step):
        for when, allowed, copy in sends:
            if when == step:
                pl.when(allowed)(copy.start)

    if hops:
        send_step(0)

    @pl.when(sp > 0)
    def _():
        halo_copy.wait_recv()
        extended[:halo_rows, :] = halo[...].astype(F32)

    @pl.when(sp == 0)
    def _():
        extended[:halo_rows, :] = jnp.zeros((halo_rows, channels), F32)


    def fold(block):
        for g in range(groups_of):
            lanes = slice(g * PAIR, (g + 1) * PAIR)
            right = spread_pair(concat([block[:HEAD, lanes], block[HEAD:, lanes]], axis=1))
            moved = dot(carried[:, lanes], right)
            local_read[:, lanes] = local_read[:, lanes] + moved[:, :PAIR]
            carried[:, lanes] = moved[:, PAIR:].astype(BF16)

    @pl.when(parity == 1)
    def _():
        fold(early_map)

    arrive("g", "hgain")
    gate = jax.nn.sigmoid(kept(project(g_buf))) * hgain[...]
    arrive("taps", "ggain", "gshift")
    tap_count = taps.shape[0]
    total = jnp.zeros((rows, channels), F32)
    for offset in range(tap_count):
        begin = halo_rows - tap_count + 1 + offset
        total = total + taps[offset:offset + 1, :] * extended[begin:begin + rows, :]
    means = jnp.where(head_blocks(channels), 1.0 / HEAD, 0.0).astype(BF16)
    centred = total - mm_left(total, means)
    scaled = centred * lax.rsqrt(mm_left(centred * centred, means) + GROUP_EPS)
    conv_out[...] = jax.nn.silu(scaled * ggain[...] + gshift[...]).astype(BF16)

    span = rows // n_tp

    def peer(step):
        if n_tp & (n_tp - 1):
            return lax.rem(tp + step, n_tp), lax.rem(tp - step + n_tp, n_tp)
        other, bit = tp, 1
        while bit < n_tp:
            if step & bit:
                other = other + bit - 2 * bit * lax.rem(tp // bit, 2)
            bit *= 2
        return other, other

    def spread(source, slots, send, recv):
        started = {}
        for step in list(range(2, n_tp, 2)) + list(range(n_tp - 1 + n_tp % 2, 0, -2)):
            if step >= n_tp:
                continue
            target = peer(step)[0]
            begin = pl.multiple_of(target * span, span)
            started[step] = pltpu.make_async_remote_copy(
                src_ref=source.at[pl.ds(begin, span)], dst_ref=slots.at[step - 1],
                send_sem=send.at[step - 1], recv_sem=recv.at[step - 1],
                device_id=(sp, target), device_id_type=MESH,
            )
            started[step].start()
        return started

    conv_copies = spread(conv_out, conv_slots, conv_send, conv_recv)

    own = pl.multiple_of(tp * span, span)

    def gather(result, source, slots, arriving, weight, depth, lanes):
        def take(result, rows, owner):
            for begin in range(0, depth, lanes):
                left = rows[:, begin:begin + lanes]
                offset = pl.multiple_of(owner * depth + begin, lanes)
                result = result + dot(left, weight[pl.ds(offset, lanes)])
            return result

        result = take(result, source[pl.ds(own, span)], tp)
        for step in range(1, n_tp):
            arriving[step].wait_recv()
            result = take(result, slots[step - 1], peer(step)[1])
        return result

    entered[...] = jnp.zeros_like(entered)
    for k, ahead in enumerate(hops):
        final = group < 2 * ahead
        following = 2 * ahead

        @pl.when(group >= ahead)
        def _():
            hop(pair_map, k, 0).wait_recv()

        @pl.when((group >= ahead) & final)
        def _():
            entered[...] = maps[k, :HEAD]

        if following < groups:
            @pl.when(group >= ahead)
            def _():
                arrived = maps[k, :HEAD].astype(F32)
                state[...] = arrived if k == 0 else chain(arrived, reach[...]) + state[...]

            @pl.when((group == 0) & (k == 0))
            def _():
                state[...] = jnp.zeros_like(state)

            @pl.when((group >= 1) & (group + following < groups))
            def _():
                windows[k + 1, :HEAD] = (
                    chain(state[...], pair_map[HEAD:]) + pair_map[:HEAD].astype(F32)
                ).astype(WIRE)

            if 2 * following < groups:
                @pl.when(group >= following)
                def _():
                    hop(pair_map, k, 1).wait_recv()
                    further = maps[k, HEAD:]
                    if k > 0:
                        further = chain(further.astype(F32), reach[...]).astype(WIRE)
                    reach[...] = further

                @pl.when((group >= following) & (group + following < groups))
                def _():
                    windows[k + 1, HEAD:] = chain(
                        reach[...].astype(F32), pair_map[HEAD:]
                    ).astype(WIRE)
            else:
                @pl.when(group >= following)
                def _():
                    hop(pair_map, k, 1).wait_recv()

            send_step(k + 1)

            @pl.when(group >= following)
            def _():
                fold(maps.at[k])

    head_means = jnp.where(head_blocks(PAIR), 1.0 / HEAD, 0.0).astype(BF16)
    lanes_of = [slice(g * PAIR, (g + 1) * PAIR) for g in range(groups_of)]
    centred = [
        local_read[:, lanes] + dot(carried[:, lanes], diagonal(part))
        for lanes, part in zip(lanes_of, by_pair(entered[...]))
    ]
    power = [dot((read * read).astype(BF16), head_means) for read in centred]
    for g, lanes in enumerate(lanes_of):
        scaled = centred[g] * lax.rsqrt(power[g] + HEAD_EPS)
        mix_out[:, lanes] = (scaled * gate[:, lanes]).astype(BF16)
    mix_copies = spread(mix_out, mix_slots, mix_send, mix_recv)
    arrive("co")
    result = gather(
        jnp.zeros(out.shape, F32), conv_out, conv_slots, conv_copies, co_buf, channels, channels
    )

    arrive("ao")
    result = gather(result, mix_out, mix_slots, mix_copies, ao_buf, width, PAIR)
    out[...] = result.astype(BF16)
    for step in range(1, n_tp):
        conv_copies[step].wait_send()
        mix_copies[step].wait_send()

    @pl.when(has_next)
    def _():
        halo_copy.wait_send()

    for _, allowed, copy in sends:
        pl.when(allowed)(copy.wait_send)

    @pl.when((group > 0) | first_member)
    def _():
        pair_part(0).wait_send()

    @pl.when(group > 0)
    def _():
        pair_part(1).wait_send()


def local(
    n_sp, n_tp,
    tokens, input_norm_gain, convolution_value_weight, convolution_gate_weight,
    depthwise_taps_weight, convolution_group_gain, convolution_group_shift,
    receptance_weight, key_weight, value_weight, decay_weight, correction_rate_weight,
    output_gate_weight, key_prenorm_gain, decay_offset_bias, position_decay_shift,
    extra_log_decay, head_norm_gain, convolution_output_weight, attention_output_weight,
):
    rows, model = tokens.shape
    channels = convolution_value_weight.shape[1]
    width = key_weight.shape[1]
    vmem = pl.BlockSpec(memory_space=pltpu.VMEM)
    anywhere = pl.BlockSpec(memory_space=pl.ANY)

    def line(values):
        return values.reshape(1, -1)

    smalls = (
        line(input_norm_gain), line(key_prenorm_gain), line(decay_offset_bias),
        depthwise_taps_weight, line(convolution_group_gain), line(convolution_group_shift),
        line(head_norm_gain),
    )
    weights = (
        convolution_value_weight, convolution_gate_weight, key_weight, receptance_weight,
        decay_weight, correction_rate_weight, value_weight, output_gate_weight,
        convolution_output_weight, attention_output_weight,
    )
    span = rows // n_tp
    halo_rows = -(-(depthwise_taps_weight.shape[0] - 1) // 16) * 16
    hop_count = max(1, (n_sp // 2 - 1).bit_length())
    dma = pltpu.SemaphoreType.DMA
    map_shape = (2 * HEAD, width)
    return pl.pallas_call(
        functools.partial(layer_kernel, n_sp, n_tp),
        name="layer",
        out_shape=pltpu.VMEM((span, model), BF16),
        in_specs=[anywhere] * 20,
        out_specs=vmem,
        scratch_shapes=[pltpu.VMEM(small.shape, F32) for small in smalls]
        + [
            pltpu.VMEM(tokens.shape, BF16),
            pltpu.VMEM(position_decay_shift.shape, F32),
            pltpu.VMEM(extra_log_decay.shape, F32),
        ]
        + [pltpu.VMEM(weight.shape, BF16) for weight in weights]
        + [
            pltpu.VMEM((rows, channels), BF16),
            pltpu.VMEM((halo_rows + rows, channels), F32),
            pltpu.VMEM((halo_rows, channels), BF16),
            pltpu.VMEM(map_shape, WIRE),
            pltpu.VMEM(map_shape, WIRE),
            pltpu.VMEM(map_shape, WIRE),
            pltpu.VMEM(map_shape, WIRE),
            pltpu.VMEM((hop_count,) + map_shape, WIRE),
            pltpu.VMEM((hop_count,) + map_shape, WIRE),
            pltpu.VMEM((HEAD, width), F32),
            pltpu.VMEM((HEAD, width), WIRE),
            pltpu.VMEM((HEAD, width), WIRE),
            pltpu.VMEM((rows, width), F32),
            pltpu.VMEM((rows, width), BF16),
            pltpu.VMEM((rows, channels), BF16),
            pltpu.VMEM((rows, width), BF16),
            pltpu.VMEM((n_tp - 1, span, channels), BF16),
            pltpu.VMEM((n_tp - 1, span, width), BF16),
            dma((11,)), dma((2,)), dma((4,)), dma((2 * hop_count - 1,)), dma((2 * hop_count - 1,)),
            dma((hop_count,)),
            dma((n_tp - 1,)), dma((n_tp - 1,)), dma((n_tp - 1,)), dma((n_tp - 1,)),
        ],
        compiler_params=pltpu.CompilerParams(
            collective_id=0, has_side_effects=True, vmem_limit_bytes=VMEM_LIMIT
        ),
    )(
        *smalls, tokens, position_decay_shift, extra_log_decay, *weights,
    )


def solution(mesh):
    in_specs = (
        P("sp", None),
        P(),
        P(None, "tp"),
        P(None, "tp"),
        P(None, "tp"),
        P("tp"),
        P("tp"),
        P(None, "tp"),
        P(None, "tp"),
        P(None, "tp"),
        P(None, "tp"),
        P(None, "tp"),
        P(None, "tp"),
        P("tp"),
        P("tp"),
        P("sp", "tp"),
        P("sp", "tp"),
        P("tp"),
        P(),
        P(),
    )
    body = functools.partial(local, mesh.shape["sp"], mesh.shape["tp"])
    return jax.shard_map(
        body, mesh=mesh, in_specs=in_specs, out_specs=P(("sp", "tp"), None), check_vma=False
    )
```

```python
import functools

import jax
import jax.numpy as jnp
from jax import lax
from jax.experimental import pallas as pl
from jax.experimental.pallas import tpu as pltpu
from jax.sharding import PartitionSpec as P

HEAD = 64
CHUNK = 64
TOKEN_PARTS = 2
PAIR = 128

NORM_EPS = 1e-06
GROUP_EPS = 1e-05
HEAD_EPS = 0.00064
KEY_EPS = 1e-06
MESH = pl.DeviceIdType.MESH
WIRE = jnp.bfloat16
VMEM_LIMIT = 60 * 1024 * 1024
F32 = jnp.float32
BF16 = jnp.bfloat16

NN = (((1,), (0,)), ((), ()))
NT = (((1,), (1,)), ((), ()))
TN = (((0,), (0,)), ((), ()))


def parts(x, count):
    out = []
    for _ in range(count - 1):
        piece = x.astype(BF16)
        out.append(piece)
        x = x - piece.astype(F32)
    out.append(x.astype(BF16))
    return out


def dot(a, b, dims=NN):
    return lax.dot_general(a, b, dims, preferred_element_type=F32)


def mm_left(a, b, dims=NN, count=2):
    pieces = [dot(piece, b, dims) for piece in parts(a, count)]
    return functools.reduce(jnp.add, pieces)


def split(x):
    high = x.astype(BF16)
    return high, (x - high.astype(F32)).astype(BF16)


def concat(pieces, axis=0):
    return jnp.concatenate(pieces, axis=axis)


def iota2(rows, cols):
    return (
        lax.broadcasted_iota(jnp.int32, (rows, cols), 0),
        lax.broadcasted_iota(jnp.int32, (rows, cols), 1),
    )


def head_blocks(width):
    row, col = iota2(width, width)
    return (row // HEAD) == (col // HEAD)


def own_head(shape):
    row, col = iota2(*shape)
    return (row // HEAD) == ((col % PAIR) // HEAD)


def diagonal(x):
    lane = lax.broadcasted_iota(jnp.int32, x.shape, 1)
    zero = jnp.zeros_like(x)
    return concat([jnp.where(lane < HEAD, x, zero), jnp.where(lane < HEAD, zero, x)])


def spread_pair(x):
    return concat([diagonal(x[:, :PAIR]), diagonal(x[:, PAIR:])], axis=1)


def compose(later, earlier):
    high, low = split(later[:, PAIR:])
    early_high, early_low = split(earlier)
    both = dot(concat([high, low]), spread_pair(early_high))
    out = both[:HEAD] + both[HEAD:] + dot(high, spread_pair(early_low))
    return concat([out[:, :PAIR] + later[:, :PAIR], out[:, PAIR:]], axis=1)


def layer_kernel(
    n_sp, n_tp,
    gain_hbm, kgain_hbm, bias_hbm, taps_hbm, ggain_hbm, gshift_hbm, hgain_hbm,
    tok_hbm, shift_hbm, extra_hbm, wcv, wcg, wk, wr, wd, we, wv, wg, wco, wao,
    out,
    gain, kgain, bias, taps, ggain, gshift, hgain,
    tok, shift, extra, cv_buf, cg_buf, k_buf, r_buf, d_buf, e_buf, v_buf, g_buf, co_buf, ao_buf,
    conv_in, extended, halo, own_map, partner_map, pair_map, early_map, maps, windows, state, reach, entered,
    local_read, carried, conv_out, mix_out, conv_slots, mix_slots,
    weight_sem, halo_sem, pair_sem, map_send, map_recv, conv_send, conv_recv, mix_send, mix_recv,
):
    sp, tp = lax.axis_index("sp"), lax.axis_index("tp")
    part = tok_hbm.shape[0] // TOKEN_PARTS
    order = dict(gain=(gain_hbm, gain))
    for index in range(TOKEN_PARTS):
        span = pl.ds(index * part, part)
        order["tok" + str(index)] = (tok_hbm.at[span], tok.at[span])
    order.update(
        k=(wk, k_buf), kgain=(kgain_hbm, kgain), d=(wd, d_buf), bias=(bias_hbm, bias),
        shift=(shift_hbm, shift), extra=(extra_hbm, extra), e=(we, e_buf), v=(wv, v_buf),
        cv=(wcv, cv_buf), cg=(wcg, cg_buf), r=(wr, r_buf), g=(wg, g_buf),
        taps=(taps_hbm, taps), ggain=(ggain_hbm, ggain), gshift=(gshift_hbm, gshift),
        hgain=(hgain_hbm, hgain), co=(wco, co_buf), ao=(wao, ao_buf),
    )
    together = (
        ("gain", "tok0"), ("tok1",), ("k", "d"), ("bias", "shift", "extra", "kgain", "e"), ("v",),
        ("cv", "cg"), ("r",), ("taps", "ggain", "gshift"), ("g", "hgain"), ("co",), ("ao",),
    )
    copies = {}
    for index, keys in enumerate(together):
        for key in keys:
            source, buffer = order[key]
            copies[key] = pltpu.make_async_copy(source, buffer, weight_sem.at[index])

    def begin(*keys):
        for key in keys:
            copies[key].start()

    def arrive(*keys):
        for key in keys:
            copies[key].wait()

    token_keys = ["tok" + str(index) for index in range(TOKEN_PARTS)]
    begin("gain", *token_keys, "k", "kgain", "d", "bias", "shift", "extra", "e", "v")
    barrier = pltpu.get_barrier_semaphore()
    for step in range(1, n_sp):
        pl.semaphore_signal(
            barrier, inc=1, device_id=(lax.rem(sp + step, n_sp), tp), device_id_type=MESH
        )
    for step in range(1, n_tp):
        pl.semaphore_signal(
            barrier, inc=1, device_id=(sp, lax.rem(tp + step, n_tp)), device_id_type=MESH
        )
    rows = tok.shape[0]
    channels = conv_in.shape[1]
    width = local_read.shape[1]
    heads = width // HEAD
    pairs = rows // PAIR
    halo_rows = halo.shape[0]
    groups = n_sp // 2
    group, parity = sp // 2, lax.rem(sp, 2)
    first_member = parity == 0
    quarters = []
    for index, key in enumerate(token_keys):
        arrive(*(("gain", key) if index == 0 else (key,)))
        x = tok[index * part:(index + 1) * part].astype(F32)
        quarters.append(
            (
                x * lax.rsqrt(jnp.mean(x * x, axis=-1, keepdims=True) + NORM_EPS) * gain[...]
            ).astype(BF16)
        )
    begin("cv", "cg", "r", "g", "taps", "ggain", "gshift", "hgain")
    middle_part = TOKEN_PARTS // 2
    halves = [concat(quarters[:middle_part]), concat(quarters[middle_part:])]
    normed = concat(halves)

    def kept(x):
        return x.astype(BF16).astype(F32)

    def project(weight):
        return concat([dot(half, weight[...]) for half in halves])

    arrive("k", "d")
    key_all, slope = kept(dot(normed, k_buf[...])), kept(dot(normed, d_buf[...]))
    arrive("bias", "shift", "extra", "kgain", "e")
    rate = kept(project(e_buf))
    same_head = head_blocks(width)
    ones = jnp.where(same_head, 1.0, 0.0).astype(BF16)
    row, col = iota2(width, width)
    centre = (jnp.where(row == col, 1.0, 0.0) - jnp.where(same_head, 1.0 / HEAD, 0.0)).astype(BF16)
    logits = slope + bias[...] + shift[...]
    decay = jax.nn.sigmoid(logits) * (-0.6065306597126334) + extra[...]
    row, col = iota2(PAIR, 2 * PAIR)
    col = col % PAIR
    tri = jnp.where(((row // CHUNK) == (col // CHUNK)) & (row >= col), 1.0, 0.0).astype(BF16)
    cum = concat(
        [dot(tri, concat(split(decay[p:p + PAIR]))) for p in range(0, rows, PAIR)]
    )
    unit = key_all * kgain[...]
    unit = unit * lax.rsqrt(dot((unit * unit).astype(BF16), ones) + KEY_EPS)
    erase = -(unit * jax.nn.sigmoid(rate))
    chunks = rows // CHUNK
    groups_of = width // PAIR

    def by_chunk(row_of):
        return concat(
            [jnp.broadcast_to(row_of(c), (CHUNK, width)) for c in range(0, rows, CHUNK)]
        )

    def middle(c):
        return cum[c + CHUNK // 2 - 1:c + CHUNK // 2]

    def last(c):
        return cum[c + CHUNK - 1:c + CHUNK]

    mid = by_chunk(middle)
    from_start = by_chunk(lambda c: jnp.exp(middle(c)))
    to_end = by_chunk(lambda c: jnp.exp(last(c) - middle(c)))
    up = jnp.exp(mid - cum)
    left_unit = unit * jnp.exp(cum - decay - mid)
    query_unit = (left_unit * from_start).astype(BF16)
    left_unit = left_unit.astype(BF16)
    right_erase, right_key = erase * up, key_all * up
    kept_erase, kept_key = (right_erase * to_end).astype(BF16), (right_key * to_end).astype(BF16)
    right_erase, right_key = right_erase.astype(BF16), right_key.astype(BF16)
    units = [(c, g) for c in range(chunks) for g in range(groups_of)]

    def piece(values, unit_index):
        c, g = unit_index
        return values[c * CHUNK:(c + 1) * CHUNK, g * PAIR:(g + 1) * PAIR]

    row, col = iota2(CHUNK, PAIR)
    col = col % CHUNK
    strict, inclusive = row > col, row >= col
    eye = jnp.where(row == col, 1.0, 0.0)
    rights = [
        concat([diagonal(piece(right_erase, u)), diagonal(piece(right_key, u))]) for u in units
    ]
    products = [dot(piece(left_unit, u), right, NT) for u, right in zip(units, rights)]
    lower = [jnp.where(strict, product[:, :PAIR], 0.0) for product in products]
    mixes = [jnp.where(strict, product[:, PAIR:], 0.0).astype(BF16) for product in products]
    arrive("v")
    begin("co", "ao")
    slices = [slice(b, b + 2 * PAIR) for b in range(0, normed.shape[1], 2 * PAIR)]
    value_sums = [None, None]

    def value_some(count):
        for span in [slices.pop(0) for _ in range(min(count, len(slices)))]:
            for index, half in enumerate(halves):
                part_of = dot(half[:, span], v_buf[span, :])
                held = value_sums[index]
                value_sums[index] = part_of if held is None else held + part_of

    def within(size):
        return (row // size) == (col // size)

    def powers(left, right):
        return dot(left, concat([diagonal(right), diagonal(left)], axis=1))

    step = [jnp.where(within(4), low, 0.0) for low in lower]
    inverse = [eye + s for s in step]
    narrow = [s.astype(BF16) for s in step]
    square = [dot(s, diagonal(s)).astype(BF16) for s in narrow]
    value_some(3)
    inverse = [
        inv + dot(s, diagonal(inv.astype(BF16))) for inv, s in zip(inverse, square)
    ]
    value_some(3)
    narrow = [inv.astype(BF16) for inv in inverse]
    step = [
        dot(inv, diagonal(jnp.where(within(16) & ~within(4), low, 0.0).astype(BF16))).astype(BF16)
        for inv, low in zip(narrow, lower)
    ]
    value_some(len(slices))
    both = [powers(s, inv) for s, inv in zip(step, narrow)]
    value_high, value_low = split(dot(concat(value_sums).astype(BF16), centre))
    inverse = [inv + pair[:, :PAIR] for inv, pair in zip(inverse, both)]
    square = [pair[:, PAIR:].astype(BF16) for pair in both]
    inverse = [
        (inv + dot(s, diagonal(inv.astype(BF16)))).astype(BF16) for inv, s in zip(inverse, square)
    ]
    value_diagonals = [
        concat([diagonal(piece(value_high, u)), diagonal(piece(value_low, u))]) for u in units
    ]
    mixed = [
        dot(concat([mix, mix], axis=1), held) for mix, held in zip(mixes, value_diagonals)
    ]
    outer = [diagonal(jnp.where(within(16), 0.0, low).astype(BF16)) for low in lower]
    step = [dot(inv, far).astype(BF16) for inv, far in zip(inverse, outer)]
    sides = [
        spread_pair(concat([mix.astype(BF16), piece(query_unit, u)], axis=1))
        for mix, u in zip(mixed, units)
    ]
    solved = [dot(inv, side) for inv, side in zip(inverse, sides)]
    square = [dot(s, diagonal(s)).astype(BF16) for s in step]
    solved = [
        part + dot(s, spread_pair(part.astype(BF16))) for s, part in zip(step, solved)
    ]
    solved = [
        (part + dot(s, spread_pair(part.astype(BF16)))).astype(BF16)
        for s, part in zip(square, solved)
    ]
    nothing = jnp.zeros((CHUNK, PAIR), BF16)
    lane = lax.broadcasted_iota(jnp.int32, (HEAD, 2 * PAIR), 1)
    first_head = (lane % PAIR) < HEAD
    blocks = {}
    for index, u in enumerate(units):
        c, g = u
        left = concat([piece(kept_erase, u), piece(kept_key, u), piece(kept_key, u)])
        right = concat(
            [
                solved[index],
                concat([piece(value_high, u), nothing], axis=1),
                concat([piece(value_low, u), nothing], axis=1),
            ]
        )
        product = dot(left, right, TN)
        product = jnp.where(first_head, product[:HEAD], product[HEAD:])
        stay = jnp.exp(last(c * CHUNK)[:, g * PAIR:(g + 1) * PAIR])
        blocks[u] = concat([product[:, :PAIR], product[:, PAIR:] + eye * stay], axis=1)
    spans = {}
    for c in range(chunks):
        for g in range(groups_of):
            spans[c, c + 1, g] = blocks[c, g]
    size = 1
    while size < chunks:
        for c in range(0, chunks, 2 * size):
            for g in range(groups_of):
                spans[c, c + 2 * size, g] = compose(
                    spans[c + size, c + 2 * size, g], spans[c, c + size, g]
                )
        size *= 2
    totals = [spans[0, chunks, g] for g in range(groups_of)]
    own_total = concat(
        [
            concat([totals[g][:, :PAIR] for g in range(groups_of)], axis=1),
            concat([totals[g][:, PAIR:] for g in range(groups_of)], axis=1),
        ]
    ).astype(WIRE)
    own_map[...] = own_total

    pl.semaphore_wait(barrier, n_sp + n_tp - 2)
    origin = group == 0
    leads = origin & first_member

    def pair_part(side):
        span_of = pl.ds(side * HEAD, HEAD)
        return pltpu.make_async_remote_copy(
            src_ref=own_map.at[span_of], dst_ref=partner_map.at[span_of],
            send_sem=pair_sem.at[2], recv_sem=pair_sem.at[side],
            device_id=(sp + 1 - 2 * parity, tp), device_id_type=MESH,
        )

    @pl.when((group > 0) | first_member)
    def _():
        pair_part(0).start()

    @pl.when(group > 0)
    def _():
        pair_part(1).start()

    arrive("cv", "cg")
    both = concat([cv_buf[...], cg_buf[...]], axis=1)
    conv_pair = kept(concat([dot(part, both) for part in halves]))
    conv_rows = (
        conv_pair[:, :channels] * jax.nn.sigmoid(conv_pair[:, channels:])
    ).astype(BF16)
    conv_in[...] = conv_rows
    halo_copy = pltpu.make_async_remote_copy(
        src_ref=conv_in.at[pl.ds(rows - halo_rows, halo_rows)], dst_ref=halo,
        send_sem=halo_sem.at[0], recv_sem=halo_sem.at[1],
        device_id=(sp + 1, tp), device_id_type=MESH,
    )
    has_next = sp + 1 < n_sp

    @pl.when(has_next)
    def _():
        halo_copy.start()

    extended[halo_rows:, :] = conv_rows.astype(F32)

    arrive("r")
    receptance = kept(project(r_buf))
    left_read = receptance * jnp.exp(cum - mid)
    query_read = left_read * from_start
    left_read = left_read.astype(BF16)
    zeros = jnp.zeros((PAIR, PAIR), BF16)
    products = [dot(piece(left_read, u), right, NT) for u, right in zip(units, rights)]
    reads = []
    for product, end, both, u in zip(products, solved, value_diagonals, units):
        keys = jnp.where(inclusive, product[:, PAIR:], 0.0).astype(BF16)
        mix = concat(
            [jnp.where(inclusive, product[:, :PAIR], 0.0).astype(BF16), keys, keys], axis=1
        )
        stacked = concat(
            [spread_pair(end), concat([both, concat([zeros, zeros])], axis=1)]
        )
        reads.append(dot(mix, stacked))
    priors = {}
    for c in range(1, chunks):
        start, size = 0, chunks // 2
        while start < c:
            while start + size > c:
                size //= 2
            for g in range(groups_of):
                block = spans[start, start + size, g]
                priors[c, g] = block if start == 0 else compose(block, priors[c, g])
            start += size
    for index, u in enumerate(units):
        c, g = u
        near, far = reads[index][:, :PAIR], reads[index][:, PAIR:] + piece(query_read, u)
        if c > 0:
            moved = dot(far.astype(BF16), spread_pair(priors[u].astype(BF16)))
            near, far = near + moved[:, :PAIR], moved[:, PAIR:]
        span = slice(c * CHUNK, (c + 1) * CHUNK)
        lanes = slice(g * PAIR, (g + 1) * PAIR)
        local_read[span, lanes] = near
        carried[span, lanes] = far.astype(BF16)

    def by_pair(x):
        return [x[:, g * PAIR:(g + 1) * PAIR] for g in range(groups_of)]

    def chain(held, move):
        out = []
        for state_part, move_part in zip(by_pair(held), by_pair(move)):
            right = concat([diagonal(piece_of) for piece_of in split(state_part)])
            out.append(dot(concat([move_part, move_part], axis=1), right))
        return concat(out, axis=1)

    early_map[...] = own_map[...]

    @pl.when(parity == 1)
    def _():
        pair_part(0).wait_recv()
        early_map[:HEAD] = partner_map[:HEAD]

    def join(lead, follow, side):
        moved = chain(lead[side * HEAD:(side + 1) * HEAD].astype(F32), follow[HEAD:])
        if side == 0:
            moved = moved + follow[:HEAD].astype(F32)
        pair_map[side * HEAD:(side + 1) * HEAD] = moved.astype(WIRE)

    @pl.when(origin & (parity == 1))
    def _():
        join(early_map, own_map, 0)

    @pl.when(group > 0)
    def _():
        pair_part(1).wait_recv()

    @pl.when((group > 0) & (parity == 1))
    def _():
        early_map[HEAD:] = partner_map[HEAD:]
        join(early_map, own_map, 0)
        join(early_map, own_map, 1)

    @pl.when((group > 0) & first_member)
    def _():
        pair_part(0).wait_recv()
        join(own_map, partner_map, 0)
        join(own_map, partner_map, 1)

    hops = []
    while 2 ** len(hops) < groups:
        hops.append(2 ** len(hops))

    def hop(source, k, side, member=parity):
        span_of = pl.ds(side * HEAD, HEAD)
        return pltpu.make_async_remote_copy(
            src_ref=source.at[span_of], dst_ref=maps.at[k, span_of],
            send_sem=map_send.at[0], recv_sem=map_recv.at[2 * k + side],
            device_id=(2 * (group + hops[k]) + member, tp), device_id_type=MESH,
        )

    def hop_across(k):
        return pltpu.make_async_remote_copy(
            src_ref=pair_map.at[pl.ds(0, HEAD)], dst_ref=maps.at[k, pl.ds(0, HEAD)],
            send_sem=map_send.at[0], recv_sem=map_recv.at[2 * k],
            device_id=(2 * hops[k], tp), device_id_type=MESH,
        )

    sends = []
    for k, ahead in enumerate(hops):
        reached = group + ahead < groups
        sends.append((0, origin & (parity == 1), hop_across(k)))
        sends.append((0, origin & (parity == 1), hop(pair_map, k, 0)))
        source = pair_map if k == 0 else windows.at[k]
        sends.append((k, reached & (group >= 1), hop(source, k, 0)))
        if 2 * ahead < groups:
            sends.append((k, reached & (group >= ahead), hop(source, k, 1)))

    def send_step(step):
        for when, allowed, copy in sends:
            if when == step:
                pl.when(allowed)(copy.start)

    if hops:
        send_step(0)

    @pl.when(sp > 0)
    def _():
        halo_copy.wait_recv()
        extended[:halo_rows, :] = halo[...].astype(F32)

    @pl.when(sp == 0)
    def _():
        extended[:halo_rows, :] = jnp.zeros((halo_rows, channels), F32)


    def fold(block):
        for g in range(groups_of):
            lanes = slice(g * PAIR, (g + 1) * PAIR)
            right = spread_pair(concat([block[:HEAD, lanes], block[HEAD:, lanes]], axis=1))
            moved = dot(carried[:, lanes], right)
            local_read[:, lanes] = local_read[:, lanes] + moved[:, :PAIR]
            carried[:, lanes] = moved[:, PAIR:].astype(BF16)

    @pl.when(parity == 1)
    def _():
        fold(early_map)

    arrive("g", "hgain")
    gate = jax.nn.sigmoid(kept(project(g_buf))) * hgain[...]
    arrive("taps", "ggain", "gshift")
    tap_count = taps.shape[0]
    total = jnp.zeros((rows, channels), F32)
    for offset in range(tap_count):
        begin = halo_rows - tap_count + 1 + offset
        total = total + taps[offset:offset + 1, :] * extended[begin:begin + rows, :]
    means = jnp.where(head_blocks(channels), 1.0 / HEAD, 0.0).astype(BF16)
    centred = total - mm_left(total, means)
    scaled = centred * lax.rsqrt(mm_left(centred * centred, means) + GROUP_EPS)
    conv_out[...] = jax.nn.silu(scaled * ggain[...] + gshift[...]).astype(BF16)

    span = rows // n_tp

    def peer(step):
        if n_tp & (n_tp - 1):
            return lax.rem(tp + step, n_tp), lax.rem(tp - step + n_tp, n_tp)
        other, bit = tp, 1
        while bit < n_tp:
            if step & bit:
                other = other + bit - 2 * bit * lax.rem(tp // bit, 2)
            bit *= 2
        return other, other

    def spread(source, slots, send, recv):
        started = {}
        for step in list(range(2, n_tp, 2)) + list(range(n_tp - 1 + n_tp % 2, 0, -2)):
            if step >= n_tp:
                continue
            target = peer(step)[0]
            begin = pl.multiple_of(target * span, span)
            started[step] = pltpu.make_async_remote_copy(
                src_ref=source.at[pl.ds(begin, span)], dst_ref=slots.at[step - 1],
                send_sem=send.at[0], recv_sem=recv.at[step - 1],
                device_id=(sp, target), device_id_type=MESH,
            )
            started[step].start()
        return started

    conv_copies = spread(conv_out, conv_slots, conv_send, conv_recv)

    own = pl.multiple_of(tp * span, span)

    def gather(result, source, slots, arriving, weight, depth, lanes):
        def take(result, rows, owner):
            for begin in range(0, depth, lanes):
                left = rows[:, begin:begin + lanes]
                offset = pl.multiple_of(owner * depth + begin, lanes)
                result = result + dot(left, weight[pl.ds(offset, lanes)])
            return result

        result = take(result, source[pl.ds(own, span)], tp)
        for step in range(1, n_tp):
            arriving[step].wait_recv()
            result = take(result, slots[step - 1], peer(step)[1])
        return result

    entered[...] = jnp.zeros_like(entered)
    for k, ahead in enumerate(hops):
        final = group < 2 * ahead
        following = 2 * ahead

        @pl.when(group >= ahead)
        def _():
            hop(pair_map, k, 0).wait_recv()

        @pl.when((group >= ahead) & final)
        def _():
            entered[...] = maps[k, :HEAD]

        if following < groups:
            @pl.when(group >= ahead)
            def _():
                arrived = maps[k, :HEAD].astype(F32)
                state[...] = arrived if k == 0 else chain(arrived, reach[...]) + state[...]

            @pl.when((group == 0) & (k == 0))
            def _():
                state[...] = jnp.zeros_like(state)

            @pl.when((group >= 1) & (group + following < groups))
            def _():
                windows[k + 1, :HEAD] = (
                    chain(state[...], pair_map[HEAD:]) + pair_map[:HEAD].astype(F32)
                ).astype(WIRE)

            if 2 * following < groups:
                @pl.when(group >= following)
                def _():
                    hop(pair_map, k, 1).wait_recv()
                    further = maps[k, HEAD:]
                    if k > 0:
                        further = chain(further.astype(F32), reach[...]).astype(WIRE)
                    reach[...] = further

                @pl.when((group >= following) & (group + following < groups))
                def _():
                    windows[k + 1, HEAD:] = chain(
                        reach[...].astype(F32), pair_map[HEAD:]
                    ).astype(WIRE)
            else:
                @pl.when(group >= following)
                def _():
                    hop(pair_map, k, 1).wait_recv()

            send_step(k + 1)

            @pl.when(group >= following)
            def _():
                fold(maps.at[k])

    head_means = jnp.where(head_blocks(PAIR), 1.0 / HEAD, 0.0).astype(BF16)
    lanes_of = [slice(g * PAIR, (g + 1) * PAIR) for g in range(groups_of)]
    centred = [
        local_read[:, lanes] + dot(carried[:, lanes], diagonal(part))
        for lanes, part in zip(lanes_of, by_pair(entered[...]))
    ]
    power = [dot((read * read).astype(BF16), head_means) for read in centred]
    for g, lanes in enumerate(lanes_of):
        scaled = centred[g] * lax.rsqrt(power[g] + HEAD_EPS)
        mix_out[:, lanes] = (scaled * gate[:, lanes]).astype(BF16)
    mix_copies = spread(mix_out, mix_slots, mix_send, mix_recv)
    arrive("co")
    result = gather(
        jnp.zeros(out.shape, F32), conv_out, conv_slots, conv_copies, co_buf, channels, channels
    )

    arrive("ao")
    result = gather(result, mix_out, mix_slots, mix_copies, ao_buf, width, PAIR)
    out[...] = result.astype(BF16)
    for step in range(1, n_tp):
        conv_copies[step].wait_send()
        mix_copies[step].wait_send()

    @pl.when(has_next)
    def _():
        halo_copy.wait_send()

    for _, allowed, copy in sends:
        pl.when(allowed)(copy.wait_send)

    @pl.when((group > 0) | first_member)
    def _():
        pair_part(0).wait_send()

    @pl.when(group > 0)
    def _():
        pair_part(1).wait_send()


def local(
    n_sp, n_tp,
    tokens, input_norm_gain, convolution_value_weight, convolution_gate_weight,
    depthwise_taps_weight, convolution_group_gain, convolution_group_shift,
    receptance_weight, key_weight, value_weight, decay_weight, correction_rate_weight,
    output_gate_weight, key_prenorm_gain, decay_offset_bias, position_decay_shift,
    extra_log_decay, head_norm_gain, convolution_output_weight, attention_output_weight,
):
    rows, model = tokens.shape
    channels = convolution_value_weight.shape[1]
    width = key_weight.shape[1]
    vmem = pl.BlockSpec(memory_space=pltpu.VMEM)
    anywhere = pl.BlockSpec(memory_space=pl.ANY)

    def line(values):
        return values.reshape(1, -1)

    smalls = (
        line(input_norm_gain), line(key_prenorm_gain), line(decay_offset_bias),
        depthwise_taps_weight, line(convolution_group_gain), line(convolution_group_shift),
        line(head_norm_gain),
    )
    weights = (
        convolution_value_weight, convolution_gate_weight, key_weight, receptance_weight,
        decay_weight, correction_rate_weight, value_weight, output_gate_weight,
        convolution_output_weight, attention_output_weight,
    )
    span = rows // n_tp
    halo_rows = -(-(depthwise_taps_weight.shape[0] - 1) // 16) * 16
    hop_count = max(1, (n_sp // 2 - 1).bit_length())
    dma = pltpu.SemaphoreType.DMA
    map_shape = (2 * HEAD, width)
    return pl.pallas_call(
        functools.partial(layer_kernel, n_sp, n_tp),
        name="layer",
        out_shape=pltpu.VMEM((span, model), BF16),
        in_specs=[anywhere] * 20,
        out_specs=vmem,
        scratch_shapes=[pltpu.VMEM(small.shape, F32) for small in smalls]
        + [
            pltpu.VMEM(tokens.shape, BF16),
            pltpu.VMEM(position_decay_shift.shape, F32),
            pltpu.VMEM(extra_log_decay.shape, F32),
        ]
        + [pltpu.VMEM(weight.shape, BF16) for weight in weights]
        + [
            pltpu.VMEM((rows, channels), BF16),
            pltpu.VMEM((halo_rows + rows, channels), F32),
            pltpu.VMEM((halo_rows, channels), BF16),
            pltpu.VMEM(map_shape, WIRE),
            pltpu.VMEM(map_shape, WIRE),
            pltpu.VMEM(map_shape, WIRE),
            pltpu.VMEM(map_shape, WIRE),
            pltpu.VMEM((hop_count,) + map_shape, WIRE),
            pltpu.VMEM((hop_count,) + map_shape, WIRE),
            pltpu.VMEM((HEAD, width), F32),
            pltpu.VMEM((HEAD, width), WIRE),
            pltpu.VMEM((HEAD, width), WIRE),
            pltpu.VMEM((rows, width), F32),
            pltpu.VMEM((rows, width), BF16),
            pltpu.VMEM((rows, channels), BF16),
            pltpu.VMEM((rows, width), BF16),
            pltpu.VMEM((n_tp - 1, span, channels), BF16),
            pltpu.VMEM((n_tp - 1, span, width), BF16),
            dma((11,)), dma((2,)), dma((3,)), dma((1,)), dma((2 * hop_count - 1,)),
            dma((1,)), dma((n_tp - 1,)), dma((1,)), dma((n_tp - 1,)),
        ],
        compiler_params=pltpu.CompilerParams(
            collective_id=0, has_side_effects=True, vmem_limit_bytes=VMEM_LIMIT
        ),
    )(
        *smalls, tokens, position_decay_shift, extra_log_decay, *weights,
    )


def solution(mesh):
    in_specs = (
        P("sp", None),
        P(),
        P(None, "tp"),
        P(None, "tp"),
        P(None, "tp"),
        P("tp"),
        P("tp"),
        P(None, "tp"),
        P(None, "tp"),
        P(None, "tp"),
        P(None, "tp"),
        P(None, "tp"),
        P(None, "tp"),
        P("tp"),
        P("tp"),
        P("sp", "tp"),
        P("sp", "tp"),
        P("tp"),
        P(),
        P(),
    )
    body = functools.partial(local, mesh.shape["sp"], mesh.shape["tp"])
    return jax.shard_map(
        body, mesh=mesh, in_specs=in_specs, out_specs=P(("sp", "tp"), None), check_vma=False
    )
```
